32 devices in a mesh: sp: 8 (over z, y), dp: 4 (over x, core).
Axes of the slice: x: 2, y: 2, z: 4, core: 2. Of those that a mesh axis runs over, the one named last changes fastest.
Arguments:
- queries: bfloat16 [4, 1024, 2048], P('dp', 'sp'), may hold values from -8 to 8
- keys: bfloat16 [4, 1024, 2048], P('dp', 'sp'), may hold values from -8 to 8
- values: bfloat16 [4, 1024, 2048], P('dp', 'sp'), may hold values from -6 to 6
- proj_weight: bfloat16 [2048, 2048], P('sp'), may hold values from -0.125 to 0.125
- residual: bfloat16 [4, 1024, 2048], P('dp', 'sp'), may hold values from -6 to 6
- norm_gain: float32 [2048], replicated, may hold values from 0.1 to 1.9
- route: int32 [4, 1024, 2], P('dp', 'sp'), may hold values from 0 to 7, all different within a row; in each aligned block of 128 rows (0 to 127, 128 to 255, ..., all dimensions but the last counted through in order) at most 64 rows name the same one
- route_weight: float32 [4, 1024, 2], P('dp', 'sp'), may hold values from 0.1 to 1
- w_gate: bfloat16 [8, 2048, 1024], P('sp'), may hold values from -0.125 to 0.125
- w_up: bfloat16 [8, 2048, 1024], P('sp'), may hold values from -0.125 to 0.125
- w_down: bfloat16 [8, 1024, 2048], P('sp'), may hold values from -0.1875 to 0.1875
Outputs:
- mixed: bfloat16 [4, 1024, 2048], P('dp', 'sp')
The draws below stay inside these ranges and needn't reach their ends.
Inputs may be any that keep to these rules, and one draw needn't show every extreme that they name: `route`: in the rows of one device no expert is named by more than 64 rows, a bound that some block reaches.
All inputs are finite; a program needn't handle non-finite values.
Results may differ from the reference program's by a relative error of at most 0.013.
Values may be sent and summed in bfloat16 or wider, within the bound.
A program may use at most 128 MiB of HBM per device.

```python
import math
import jax
import jax.numpy as jnp
import numpy as np
from jax import lax

D = 2048
HEADS = 16
HEAD_DIM = 128
FFE = 1024
SEQ_DEV = 128
EXPERTS = 8
LENGTH = 1024
SEQS = 4
CAP = 64
N_SP = 8
N_DP = 4


def head_plan(key):
    first, second, third = jax.random.split(jax.random.fold_in(key, 7), 3)
    direction = jnp.where(jax.random.bernoulli(first, 0.5, (HEADS, HEAD_DIM)), 1.0, -1.0).astype(jnp.float32)
    slow = jax.random.bernoulli(second, 0.5, (HEADS,))
    level = jnp.where(slow, -jnp.log(1.0 * LENGTH) - 1.5, -jnp.log(100.0))
    drift = jax.random.uniform(third, (SEQS, LENGTH // 64, HEADS), jnp.float32, -0.8, 0.8)
    drift = jnp.repeat(drift, 64, axis=1)
    return (direction, level[None, None, :] + drift)


def noise(key):
    sample = jnp.clip(jax.random.normal(key, (SEQS, LENGTH, HEADS, HEAD_DIM), jnp.float32), -6.0, 6.0)
    return sample


def draw_keys(key, part):
    direction, level = head_plan(key)
    sample = noise(jax.random.fold_in(key, 11)) + direction[None, None, :, :]
    return sample.reshape(SEQS, LENGTH, HEADS * HEAD_DIM).astype(jnp.bfloat16)


def draw_queries(key, part):
    direction, level = head_plan(key)
    factor = level / jnp.sqrt(1.0 * HEAD_DIM)
    sample = noise(jax.random.fold_in(key, 13)) + factor[..., None] * direction[None, None, :, :]
    return sample.reshape(SEQS, LENGTH, HEADS * HEAD_DIM).astype(jnp.bfloat16)


def shard_levels(own_key, extent, pieces, low, high):
    gain, own = 1.0, jax.random.fold_in(own_key, 6)
    for dim, blocks in pieces:
        heights = jnp.exp(jax.random.uniform(jax.random.fold_in(own, dim), (blocks,), jnp.float32, low / len(pieces), high / len(pieces)))
        gain = gain * jnp.repeat(heights, extent[dim] // blocks).reshape([-1 if axis == dim else 1 for axis in range(len(extent))])
    return gain


def assign_block(stream_key, own, number, rows, amount, top, most, lean):
    order = jax.random.permutation(stream_key, amount)
    packed, common = portions_of(amount, rows * top, most, lean, True), portions_of(amount, rows * top, most, lean, False)
    places = jnp.arange(amount)

    def named(sizes, offset_by):
        used = int((sizes > 0).sum())
        fixed = max(1, used // 4)
        passed = fixed + (places - fixed + offset_by * (used - fixed)) % max(1, amount - fixed)
        return jnp.zeros((amount,), jnp.int32).at[order[jnp.where(places < fixed, places, passed)]].set(jnp.asarray(sizes, jnp.int32))

    sizes = jnp.where(number % 4 == 0, named(packed, number // 4), named(common, number - number // 4 - 1))
    mixed = jax.random.permutation(jax.random.fold_in(own, 3), amount)
    giver, receiver = mixed[0:amount // 2 * 2:2], mixed[1:amount // 2 * 2:2]
    margin = jnp.minimum(sizes[giver] - 1, most - sizes[receiver]) // 2
    margin = jnp.where((giver == order[0]) | (receiver == order[0]) | (sizes[receiver] == 0), 0, jnp.maximum(margin, 0))
    passed = jax.random.randint(jax.random.fold_in(own, 4), (amount // 2,), 0, 1 << 20) % (margin + 1)
    sizes = sizes.at[giver].add(-passed).at[receiver].add(passed)
    items = jnp.searchsorted(jnp.cumsum(sizes), jnp.arange(rows * top), side="right").astype(jnp.int32)
    grid = items.reshape(top, rows).T
    grid = grid[jax.random.permutation(jax.random.fold_in(own, 1), rows)]
    offset_by = jax.random.randint(jax.random.fold_in(own, 2), (rows, 1), 0, top)
    return jnp.take_along_axis(grid, (jnp.arange(top)[None, :] + offset_by) % top, axis=1)


def portions_of(count, total, reach, skew, full):
    loads = [(1 << 20) // math.isqrt(standing ** skew) + 1 for standing in range(1, count + 1)]
    largest = reach if full else min(reach, max(-(-total // count), total * loads[0] // sum(loads)))
    least = 1 if total - largest >= count - 1 else 0
    holding, surplus = [largest] + [least] * (count - 1), total - largest - least * (count - 1)
    while surplus > 0:
        movable = [i for i in range(1, count) if holding[i] < largest] or [i for i in range(1, count) if holding[i] < reach]
        whole, budget = sum([loads[i] for i in movable]), surplus
        for i in movable:
            extra = min(reach - holding[i], max(1, budget * loads[i] // whole), surplus)
            holding[i] = holding[i] + extra
            surplus = surplus - extra
    return np.array(holding)


def bell_draw(rng, extent, spread, most, shards=(), held_as=jnp.bfloat16):
    drawn = spread * jax.random.normal(rng, extent, jnp.float32)
    if shards:
        drawn = drawn * shard_levels(rng, extent, shards, -0.22, 0.18)
    return jnp.clip(drawn, -most, most).astype(held_as)


def setup_inputs(seed: int = 0) -> dict:
    splits = jax.random.split(jax.random.key(seed), 12)
    queries = draw_queries(jax.random.fold_in(splits[11], 71), 0)
    keys = draw_keys(jax.random.fold_in(splits[11], 71), 0)
    values = bell_draw(splits[2], (SEQS, LENGTH, D), 1.0, 6.0, ((0, 4), (1, 8)))
    proj_weight = bell_draw(splits[3], (D, D), D ** -0.5, 0.125, ((0, 8),))
    residual = bell_draw(splits[4], (SEQS, LENGTH, D), 1.0, 6.0, ((0, 4), (1, 8)))
    norm_gain = jnp.clip(1.0 + 0.18 * jax.random.normal(splits[5], (D,), jnp.float32), 0.1, 1.9)
    route_keys = jax.random.split(jax.random.fold_in(splits[6], 1), SEQS * LENGTH // SEQ_DEV)
    route_turns = jax.random.permutation(jax.random.fold_in(splits[6], 3), SEQS * LENGTH // SEQ_DEV)
    route = jax.vmap(lambda own, number: assign_block(jax.random.fold_in(splits[6], 2), own, number, SEQ_DEV, EXPERTS, 2, CAP, 2))(route_keys, route_turns).reshape((SEQS, LENGTH, 2))
    route_weight = jnp.clip(0.1 + 0.9 * jax.random.uniform(splits[7], (SEQS, LENGTH, 2), jnp.float32) ** shard_levels(splits[7], (SEQS, LENGTH, 2), ((0, 4), (1, 8)), -0.2, 0.2), 0.1, 1.0)
    w_gate = bell_draw(splits[8], (EXPERTS, D, FFE), D ** -0.5, 0.125, ((0, 8),))
    w_up = bell_draw(splits[9], (EXPERTS, D, FFE), D ** -0.5, 0.125, ((0, 8),))
    w_down = bell_draw(splits[10], (EXPERTS, FFE, D), FFE ** -0.5, 0.1875, ((0, 8),))
    return {"queries": queries, "keys": keys, "values": values, "proj_weight": proj_weight, "residual": residual, "norm_gain": norm_gain, "route": route, "route_weight": route_weight, "w_gate": w_gate, "w_up": w_up, "w_down": w_down}


EPS = 1e-06

def one_head(args):
    query, key, value = args
    length = query.shape[0]
    scores = jnp.dot(query, key.T, preferred_element_type=jnp.float32) * HEAD_DIM ** (-0.5)
    position = jnp.arange(length)
    causal = position[None, :] < position[:, None]
    softer = jnp.where(causal, jax.nn.softplus(scores), 0.0)
    suffix = lax.cumsum(softer, axis=1, reverse=True)
    weight = jnp.exp(jnp.where(causal, scores - suffix, -jnp.inf)).astype(jnp.bfloat16)
    return jnp.dot(weight, value, preferred_element_type=jnp.float32).astype(jnp.bfloat16)

def by_heads(array):
    seqs, length, width = array.shape
    heads = width // HEAD_DIM
    return array.reshape(seqs, length, heads, HEAD_DIM).transpose(0, 2, 1, 3).reshape(seqs * heads, length, HEAD_DIM)

def reference(queries, keys, values, proj_weight, residual, norm_gain, route, route_weight, w_gate, w_up, w_down):
    seqs, length, width = queries.shape
    heads = width // HEAD_DIM
    attended = lax.map(one_head, (by_heads(queries), by_heads(keys), by_heads(values)))
    attended = attended.reshape(seqs, heads, length, HEAD_DIM).transpose(0, 2, 1, 3).reshape(seqs * length, width)
    projected = jnp.dot(attended, proj_weight, preferred_element_type=jnp.float32)
    stream = (residual.reshape(seqs * length, width).astype(jnp.float32) + projected).astype(jnp.bfloat16)
    stream_f = stream.astype(jnp.float32)
    normed = (stream_f * lax.rsqrt(lax.optimization_barrier(jnp.mean(stream_f * stream_f, axis=-1, keepdims=True)) + EPS) * norm_gain).astype(jnp.bfloat16)
    flat_route = route.reshape(seqs * length, 2)
    flat_weight = route_weight.reshape(seqs * length, 2)
    bound = CAP * N_SP * N_DP

    def per_expert(total, inputs):
        expert, gate_w, up_w, down_w = inputs
        named = flat_route == expert
        scale = lax.optimization_barrier(jnp.sum(jnp.where(named, flat_weight, 0.0), axis=1))
        used = jnp.any(named, axis=1)
        index = jnp.nonzero(used, size=bound, fill_value=0)[0]
        valid = jnp.arange(bound) < jnp.sum(used.astype(jnp.int32))
        rows = normed[index]
        gate = jnp.dot(rows, gate_w, preferred_element_type=jnp.float32)
        upper = jnp.dot(rows, up_w, preferred_element_type=jnp.float32)
        hidden = (jax.nn.silu(gate) * upper).astype(jnp.bfloat16)
        result = jnp.dot(hidden, down_w, preferred_element_type=jnp.float32).astype(jnp.bfloat16)
        addend = jnp.where(valid[:, None], scale[index][:, None] * result.astype(jnp.float32), 0.0)
        return (total.at[index].add(addend), None)
    experts = w_gate.shape[0]
    total, unused = lax.scan(per_expert, stream.astype(jnp.float32), (jnp.arange(experts).astype(jnp.int32), w_gate, w_up, w_down))
    return total.astype(jnp.bfloat16).reshape(seqs, length, width)
```

```python
import functools
import math

import jax
import jax.numpy as jnp
from jax import lax
from jax.experimental import pallas as pl
from jax.experimental.pallas import tpu as pltpu
from jax.sharding import PartitionSpec as P

HEADS = 16


EPS = 1e-06

MESH = pl.DeviceIdType.MESH


def flipped(number, off, n):
    result = number
    bit = 1
    while bit < n:
        result = result + bit * lax.rem(off // bit, 2) * (1 - 2 * lax.rem(number // bit, 2))
        bit *= 2
    return result


def layer_kernel(
    n, m, ny,
    q_hbm, k_hbm, v_hbm, proj_hbm, res_hbm, gain_hbm, route_hbm, share_hbm, gate_hbm, up_hbm, down_hbm,
    out_ref,
    qbuf, kbuf, vbuf, wbuf, osend, obuf, weight_ref, carry_ref, acc, stream_ref, normed_ref,
    res_ref, gain_ref, route_ref, share_ref, info, cols_ref,
    gate_ref, up_ref, down_ref, outgoing, inbox, outbox, back,
    load_sem, own_sem,
    in_send, in_recv, o_send, o_recv, w_send, w_recv, there_send, there_recv, back_send, back_recv,
):
    me, dp = lax.axis_index("sp"), lax.axis_index("dp")
    nz = n // ny
    z, y = me // ny, lax.rem(me, ny)
    cores = 2
    nx = m // cores
    x, core = dp // cores, lax.rem(dp, cores)
    rows, width = stream_ref.shape
    cols = width // n
    head = width // HEADS
    heads_here = cols // head
    wcols = wbuf.shape[3]
    capacity = inbox.shape[1]
    pairs = n // 2
    bf16, f32 = jnp.bfloat16, jnp.float32

    def peer(sp, d):
        return {"sp": sp, "dp": d}

    def my_cols(d):
        return pl.ds(pl.multiple_of(d * cols, cols), cols)

    def row_block(d):
        return pl.ds(pl.multiple_of(d * rows, rows), rows)

    trio = ((k_hbm, kbuf), (q_hbm, qbuf), (v_hbm, vbuf))

    own = [pltpu.make_async_copy(route_hbm, route_ref, own_sem.at[0]),
           pltpu.make_async_copy(share_hbm, share_ref, own_sem.at[1])]
    own += [
        pltpu.make_async_copy(
            proj_hbm.at[:, pl.ds(q * wcols, wcols)], wbuf.at[q, me], own_sem.at[2 + q]
        )
        for q in range(m)
    ]
    own += [
        pltpu.make_async_copy(ref.at[:, my_cols(me)], buf.at[row_block(me), :], own_sem.at[2 + m + t])
        for t, (ref, buf) in enumerate(trio)
    ]
    loads = [
        pltpu.make_async_copy(res_hbm, res_ref, load_sem.at[3]),
        pltpu.make_async_copy(gain_hbm, gain_ref, load_sem.at[4]),
        pltpu.make_async_copy(gate_hbm.at[0], gate_ref, load_sem.at[0]),
        pltpu.make_async_copy(up_hbm.at[0], up_ref, load_sem.at[1]),
        pltpu.make_async_copy(down_hbm.at[0], down_ref, load_sem.at[2]),
    ]
    for copy in own:
        copy.start()

    barrier = pltpu.get_barrier_semaphore()
    for off in range(1, n):
        pl.semaphore_signal(barrier, inc=1, device_id=peer(lax.rem(me + off, n), dp), device_id_type=MESH)
    for off in range(1, m):
        pl.semaphore_signal(barrier, inc=1, device_id=peer(me, lax.rem(dp + off, m)), device_id_type=MESH)
    pl.semaphore_wait(barrier, n - 1 + m - 1)

    def in_copy(t, off):
        ref, buf = trio[t]
        to = lax.rem(me + off, n)
        return pltpu.make_async_remote_copy(
            src_ref=ref.at[:, my_cols(to)], dst_ref=buf.at[row_block(me), :],
            send_sem=in_send.at[t, off], recv_sem=in_recv.at[t, me],
            device_id=peer(to, dp), device_id_type=MESH,
        )

    def in_start(t):
        for off in range(1, n):
            in_copy(t, off).start()

    def in_wait(t, origin):
        ref, buf = trio[t]

        @pl.when(me != origin)
        def _():
            pltpu.make_async_remote_copy(
                src_ref=ref.at[:, my_cols(0)], dst_ref=buf.at[row_block(origin), :],
                send_sem=in_send.at[t, 0], recv_sem=in_recv.at[t, origin],
                device_id=peer(origin, dp), device_id_type=MESH,
            ).wait_recv()

    sent = []

    def w_start(cond, q, i, dev, own=False):
        slot = len(sent)
        source = proj_hbm.at[:, pl.ds(pl.multiple_of(q * wcols, wcols), wcols)] if own else wbuf.at[q, i]
        copy = pltpu.make_async_remote_copy(
            src_ref=source, dst_ref=wbuf.at[q, i],
            send_sem=w_send.at[slot], recv_sem=w_recv.at[q, i],
            device_id=dev, device_id_type=MESH,
        )
        sent.append((cond, copy))
        if cond is None:
            copy.start()
        else:
            pl.when(cond)(copy.start)

    def w_wait(cond, q, i):
        copy = pltpu.make_async_remote_copy(
            src_ref=wbuf.at[q, i], dst_ref=wbuf.at[q, i],
            send_sem=w_send.at[0], recv_sem=w_recv.at[q, i],
            device_id=peer(me, lax.rem(dp + 1, m)), device_id_type=MESH,
        )
        if cond is None:
            copy.wait_recv()
        else:
            pl.when(cond)(copy.wait_recv)

    up, down = z + 1 < nz, z > 0
    above, below = jnp.minimum(z + 1, nz - 1) * ny + y, jnp.maximum(z - 1, 0) * ny + y
    other = x * cores + lax.rem(core + 1, cores)

    def across(cond, i):
        for o in range(1, nx):
            w_start(cond, dp, i, peer(me, lax.rem(x + o, nx) * cores + core), False)
        w_start(cond, dp, i, peer(me, other), False)

    def column(dz, upward):
        far = z - dz if upward else z + dz
        cond = far >= 0 if upward else far < nz
        far = jnp.clip(far, 0, nz - 1)
        i = far * ny + y
        w_wait(cond, dp, i)
        more = jnp.logical_and(cond, up if upward else down)
        if dz < nz - 1:
            w_start(more, dp, i, peer(above if upward else below, dp))
        for o in range(1, ny):
            w_start(cond, dp, i, peer(z * ny + lax.rem(y + o, ny), dp))
        across(cond, i)

    def side(dz, upward, o):
        far = z - dz if upward else z + dz
        cond = (far >= 0 if upward else far < nz) if dz else None
        far = jnp.clip(far, 0, nz - 1)
        i = far * ny + lax.rem(y + o, ny)
        w_wait(cond, dp, i)
        across(cond, i)

    def beyond(off, o):
        i = lax.rem(me + off, n)
        q = lax.rem(x + o, nx) * cores + core
        w_wait(None, q, i)
        w_start(None, q, i, peer(me, other))

    def columns(dz):
        column(dz, True)
        column(dz, False)

    def sides(dz):
        for o in range(1, ny):
            side(dz, True, o)
            if dz:
                side(dz, False, o)

    w_start(up, dp, me, peer(above, dp), True)
    w_start(down, dp, me, peer(below, dp), True)
    for o in range(1, ny):
        w_start(None, dp, me, peer(z * ny + lax.rem(y + o, ny), dp), True)
    in_start(0)
    for load in loads:
        load.start()

    own[0].wait()
    own[1].wait()
    row_id = lax.broadcasted_iota(jnp.int32, (rows, rows), 0)
    col_id = lax.broadcasted_iota(jnp.int32, (rows, rows), 1)
    expert_id = lax.broadcasted_iota(jnp.int32, (n, rows), 0)
    named = [(route_ref[k : k + 1, :] == expert_id).astype(f32) for k in range(2)]
    before = jnp.dot(
        (named[0] + named[1]).astype(bf16), (row_id < col_id).astype(bf16), preferred_element_type=f32
    )
    facts = [
        route_ref[k : k + 1, :].astype(f32) * capacity + jnp.sum(named[k] * before, axis=0, keepdims=True)
        for k in range(2)
    ] + [share_ref[0:1, :], share_ref[1:2, :]]
    for k in range(4):
        info[k : k + 1, :] = facts[k]
    spread = jnp.zeros((rows, rows), f32)
    for k in range(4):
        spread = jnp.where(row_id == k, facts[k], spread)
    cols_ref[...] = spread.T

    sides(0)
    columns(1)
    in_start(1)
    sides(1)
    if nz > 2:
        columns(2)
    in_start(2)
    if nz > 2:
        sides(2)

    scale = math.log2(math.e) / math.sqrt(head)
    later = (row_id > col_id).astype(bf16)
    half = jnp.concatenate([later, jnp.ones((rows, rows), bf16)], axis=1)
    summing = jnp.concatenate([half, half], axis=0)
    log2e = math.log2(math.e)
    chunk = 2 * rows

    for copy in own[2:]:
        copy.wait()

    def weigh(b):
        for h in range(heads_here):
            lanes = slice(h * head, (h + 1) * head)
            key = kbuf[b * rows : (b + 1) * rows, lanes]
            for start in range(b * rows, n * rows, chunk):
                stop = min(start + chunk, n * rows)
                score = lax.dot_general(
                    qbuf[start:stop, lanes], key, (((1,), (1,)), ((), ())), preferred_element_type=f32
                ) * scale
                tail = jnp.log(1.0 + jnp.exp2(-jnp.abs(score))) * log2e
                soft = jnp.maximum(score, 0.0) + tail
                log_sigmoid = jnp.minimum(score, 0.0) - tail
                if start == b * rows:
                    inside = lax.broadcasted_iota(jnp.int32, soft.shape, 1) < lax.broadcasted_iota(
                        jnp.int32, soft.shape, 0
                    )
                    soft = jnp.where(inside, soft, 0.0)
                high = soft.astype(bf16)
                low = (soft - high.astype(f32)).astype(bf16)
                sums = jnp.dot(jnp.concatenate([high, low], axis=1), summing, preferred_element_type=f32)
                part = log_sigmoid - sums[:, :rows]
                fresh = rows if start == b * rows else 0
                if fresh < stop - start:
                    carry = carry_ref[h, start + fresh : stop, :]
                    if fresh:
                        carry = jnp.concatenate([jnp.zeros((fresh, rows), f32), carry], axis=0)
                    part = part - carry
                    total = sums[:, rows:] + carry
                else:
                    total = sums[:, rows:]
                weight = jnp.exp2(part)
                if start == b * rows:
                    weight = jnp.where(inside, weight, 0.0)
                weight_ref[h, start:stop, b * rows : (b + 1) * rows] = weight.astype(bf16)
                if b > 0:
                    carry_ref[h, start:stop, :] = total

    for b in range(n - 1, -1, -1):
        in_wait(0, b)
        in_wait(1, b)
        weigh(b)
    for dz in range(3, nz):
        columns(dz)
        sides(dz)

    def o_copy(d):
        return pltpu.make_async_remote_copy(
            src_ref=osend.at[d], dst_ref=obuf.at[me],
            send_sem=o_send.at[d], recv_sem=o_recv.at[me],
            device_id=peer(d, dp), device_id_type=MESH,
        )

    for d in range(n):
        in_wait(2, d)
        for h in range(heads_here):
            lanes = slice(h * head, (h + 1) * head)
            osend[d, :, lanes] = jnp.dot(
                weight_ref[h, d * rows : (d + 1) * rows, : (d + 1) * rows],
                vbuf[: (d + 1) * rows, lanes],
                preferred_element_type=f32,
            ).astype(bf16)

        @pl.when(me == d)
        def _():
            obuf[me] = osend[d]

        @pl.when(me != d)
        def _():
            o_copy(d).start()

    for off in range(1, n):
        for o in range(1, nx):
            beyond(off, o)
    for off in range(1, n):
        i = lax.rem(me + off, n)
        for x_off in range(nx):
            w_wait(None, lax.rem(x + x_off, nx) * cores + lax.rem(core + 1, cores), i)
    for load in loads:
        load.wait()

    acc[...] = res_ref[...].astype(f32)

    @pl.loop(0, n)
    def _(step):
        origin = flipped(me, step, n)

        @pl.when(step > 0)
        def _():
            pltpu.make_async_remote_copy(
                src_ref=osend.at[0], dst_ref=obuf.at[origin],
                send_sem=o_send.at[0], recv_sem=o_recv.at[origin],
                device_id=peer(origin, dp), device_id_type=MESH,
            ).wait_recv()

        block = obuf[origin]
        for q in range(m):
            part = slice(q * wcols, (q + 1) * wcols)
            acc[:, part] += jnp.dot(block, wbuf[q, origin], preferred_element_type=f32)

    square = jnp.zeros((rows, 1), f32)
    for q in range(m):
        part = slice(q * wcols, (q + 1) * wcols)
        stream = acc[:, part].astype(bf16)
        stream_ref[:, part] = stream
        stream = stream.astype(f32)
        acc[:, part] = stream
        square = square + jnp.sum(stream * stream, axis=1, keepdims=True)
    factor = lax.rsqrt(square / width + EPS)
    for q in range(m):
        part = slice(q * wcols, (q + 1) * wcols)
        normed_ref[:, part] = (acc[:, part] * factor * gain_ref[:, part]).astype(bf16)

    def gathered(expert):
        slot = lax.broadcasted_iota(jnp.int32, (capacity, rows), 0) + expert * capacity
        slot = slot.astype(f32)
        chosen = jnp.logical_or(info[0:1, :] == slot, info[1:2, :] == slot)
        return jnp.dot(chosen.astype(bf16), normed_ref[...], preferred_element_type=f32).astype(bf16)

    def there(off):
        return pltpu.make_async_remote_copy(
            src_ref=outgoing.at[off], dst_ref=inbox.at[off],
            send_sem=there_send.at[off], recv_sem=there_recv.at[off],
            device_id=peer(flipped(me, off, n), dp), device_id_type=MESH,
        )

    def home(off):
        return pltpu.make_async_remote_copy(
            src_ref=outbox.at[off], dst_ref=back.at[off],
            send_sem=back_send.at[off], recv_sem=back_recv.at[off],
            device_id=peer(flipped(me, off, n), dp), device_id_type=MESH,
        )

    @pl.loop(1, n)
    def _(off):
        outgoing[off] = gathered(flipped(me, off, n))
        there(off).start()

    inbox[0] = gathered(me)

    hidden_width = gate_ref.shape[1]
    piece = min(512, hidden_width)

    @pl.loop(0, pairs)
    def _(pair):
        @pl.when(pair > 0)
        def _():
            there(pair * 2).wait_recv()

        there(pair * 2 + 1).wait_recv()
        arrived = inbox[pl.ds(pair * 2, 2)].reshape(2 * capacity, width)
        hidden = []
        for first in range(0, hidden_width, piece):
            part = slice(first, first + piece)
            gate = jnp.dot(arrived, gate_ref[:, part], preferred_element_type=f32)
            upper = jnp.dot(arrived, up_ref[:, part], preferred_element_type=f32)
            hidden.append((jax.nn.silu(gate) * upper).astype(bf16))
        hidden = jnp.concatenate(hidden, axis=1)
        for first in range(0, width, piece):
            part = slice(first, first + piece)
            result = jnp.dot(hidden, down_ref[:, part], preferred_element_type=f32)
            outbox[pl.ds(pair * 2, 2), :, part] = result.astype(bf16).reshape(2, capacity, piece)

        @pl.when(pair > 0)
        def _():
            home(pair * 2).start()

        @pl.when(pair == 0)
        def _():
            back[0] = outbox[0]

        home(pair * 2 + 1).start()

    @pl.loop(0, pairs)
    def _(pair):
        @pl.when(pair > 0)
        def _():
            home(pair * 2).wait_recv()

        home(pair * 2 + 1).wait_recv()
        slot = lax.broadcasted_iota(jnp.int32, (rows, 2 * capacity), 1)
        even, odd = flipped(me, pair * 2, n), flipped(me, pair * 2 + 1, n)
        slot = jnp.where(slot < capacity, slot + even * capacity, slot - capacity + odd * capacity)
        slot = slot.astype(f32)
        first = (cols_ref[:, 0:1] == slot).astype(bf16)
        second = (cols_ref[:, 1:2] == slot).astype(bf16)
        for start in range(0, width, piece):
            part = slice(start, start + piece)
            block = back[pl.ds(pair * 2, 2), :, part].reshape(2 * capacity, piece)
            acc[:, part] += cols_ref[:, 2:3] * jnp.dot(
                first, block, preferred_element_type=f32
            ) + cols_ref[:, 3:4] * jnp.dot(second, block, preferred_element_type=f32)

    out_ref[...] = acc[...].astype(bf16)

    for t in range(3):
        for off in range(1, n):
            in_copy(t, off).wait_send()
    for d in range(n):
        @pl.when(me != d)
        def _():
            o_copy(d).wait_send()
    for cond, copy in sent:
        if cond is None:
            copy.wait_send()
        else:
            pl.when(cond)(copy.wait_send)

    @pl.loop(1, n)
    def _(off):
        there(off).wait_send()
        home(off).wait_send()


def layer(queries, keys, values, proj_weight, residual, norm_gain, route, share, w_gate, w_up, w_down):
    n, m = lax.axis_size("sp"), lax.axis_size("dp")
    rows, width = queries.shape
    cols = width // n
    ny = 1 << ((n.bit_length() - 1) // 2)
    nz, nx = n // ny, m // 2
    copies = 1 + ny + 2 * nz * (ny + nx + 1) + (2 * nz) * ny * nx + n * nx
    capacity = 4 * rows // n
    hidden = w_gate.shape[2]
    heads_here = cols // (width // HEADS)
    bf16, f32 = jnp.bfloat16, jnp.float32
    return pl.pallas_call(
        functools.partial(layer_kernel, n, m, ny),
        out_shape=jax.ShapeDtypeStruct((rows, width), bf16),
        in_specs=[pl.BlockSpec(memory_space=pl.ANY)] * 11,
        out_specs=pl.BlockSpec(memory_space=pltpu.VMEM),
        scratch_shapes=[
            pltpu.VMEM((n * rows, cols), bf16),
            pltpu.VMEM((n * rows, cols), bf16),
            pltpu.VMEM((n * rows, cols), bf16),
            pltpu.VMEM((m, n, cols, width // m), bf16),
            pltpu.VMEM((n, rows, cols), bf16),
            pltpu.VMEM((n, rows, cols), bf16),
            pltpu.VMEM((heads_here, n * rows, n * rows), bf16),
            pltpu.VMEM((heads_here, n * rows, rows), f32),
            pltpu.VMEM((rows, width), f32),
            pltpu.VMEM((rows, width), bf16),
            pltpu.VMEM((rows, width), bf16),
            pltpu.VMEM((rows, width), bf16),
            pltpu.VMEM((1, width), f32),
            pltpu.VMEM((2, rows), jnp.int32),
            pltpu.VMEM((2, rows), f32),
            pltpu.VMEM((8, rows), f32),
            pltpu.VMEM((rows, rows), f32),
            pltpu.VMEM((width, hidden), bf16),
            pltpu.VMEM((width, hidden), bf16),
            pltpu.VMEM((hidden, width), bf16),
            pltpu.VMEM((n, capacity, width), bf16),
            pltpu.VMEM((n, capacity, width), bf16),
            pltpu.VMEM((n, capacity, width), bf16),
            pltpu.VMEM((n, capacity, width), bf16),
            pltpu.SemaphoreType.DMA((5,)),
            pltpu.SemaphoreType.DMA((5 + m,)),
            pltpu.SemaphoreType.DMA((3, n)),
            pltpu.SemaphoreType.DMA((3, n)),
            pltpu.SemaphoreType.DMA((n,)),
            pltpu.SemaphoreType.DMA((n,)),
            pltpu.SemaphoreType.DMA((copies,)),
            pltpu.SemaphoreType.DMA((m, n)),
            pltpu.SemaphoreType.DMA((n,)),
            pltpu.SemaphoreType.DMA((n,)),
            pltpu.SemaphoreType.DMA((n,)),
            pltpu.SemaphoreType.DMA((n,)),
        ],
        compiler_params=pltpu.CompilerParams(
            collective_id=0, has_side_effects=True, vmem_limit_bytes=56 * 1024 * 1024
        ),
    )(
        queries, keys, values, proj_weight, residual, norm_gain.reshape(1, width),
        route.T, share.T, w_gate, w_up, w_down,
    )


def body(
    queries,
    keys,
    values,
    proj_weight,
    residual,
    norm_gain,
    route,
    route_weight,
    w_gate,
    w_up,
    w_down,
):
    return layer(
        queries[0], keys[0], values[0], proj_weight, residual[0], norm_gain,
        route[0], route_weight[0], w_gate, w_up, w_down,
    )[None]


def solution(mesh):
    return jax.shard_map(
        body,
        mesh=mesh,
        in_specs=(
            P("dp", "sp", None),
            P("dp", "sp", None),
            P("dp", "sp", None),
            P("sp", None),
            P("dp", "sp", None),
            P(),
            P("dp", "sp", None),
            P("dp", "sp", None),
            P("sp", None, None),
            P("sp", None, None),
            P("sp", None, None),
        ),
        out_specs=P("dp", "sp", None),
        check_vma=False,
    )
```

```python
import functools
import math

import jax
import jax.numpy as jnp
from jax import lax
from jax.experimental import pallas as pl
from jax.experimental.pallas import tpu as pltpu
from jax.sharding import PartitionSpec as P

HEADS = 16


EPS = 1e-06

MESH = pl.DeviceIdType.MESH


def flipped(number, off, n):
    result = number
    bit = 1
    while bit < n:
        result = result + bit * lax.rem(off // bit, 2) * (1 - 2 * lax.rem(number // bit, 2))
        bit *= 2
    return result


def layer_kernel(
    n, m, ny,
    q_hbm, k_hbm, v_hbm, proj_hbm, res_hbm, gain_hbm, route_hbm, share_hbm, gate_hbm, up_hbm, down_hbm,
    out_ref,
    qbuf, kbuf, vbuf, wbuf, osend, obuf, weight_ref, carry_ref, acc, stream_ref, normed_ref,
    res_ref, gain_ref, route_ref, share_ref, info, cols_ref,
    gate_ref, up_ref, down_ref, outgoing, inbox, outbox, back,
    raw_ref, relay_out, relay_in, partial_ref, part_ref, mate_info, mate_cols,
    load_sem, own_sem,
    in_send, in_recv, o_send, o_recv, w_send, w_recv, there_send, there_recv, back_send, back_recv,
    info_sem, raw_sem, relay_send, via_recv, part_sem,
):
    me, dp = lax.axis_index("sp"), lax.axis_index("dp")
    nz = n // ny
    z, y = me // ny, lax.rem(me, ny)
    cores = 2
    nx = m // cores
    x, core = dp // cores, lax.rem(dp, cores)
    rows, width = stream_ref.shape
    cols = width // n
    head = width // HEADS
    heads_here = cols // head
    wcols = wbuf.shape[3]
    capacity = inbox.shape[1]
    pairs = n // 2
    bf16, f32 = jnp.bfloat16, jnp.float32

    def peer(sp, d):
        return {"sp": sp, "dp": d}

    def my_cols(d):
        return pl.ds(pl.multiple_of(d * cols, cols), cols)

    def row_block(d):
        return pl.ds(pl.multiple_of(d * rows, rows), rows)

    trio = ((k_hbm, kbuf), (q_hbm, qbuf), (v_hbm, vbuf))

    own = [pltpu.make_async_copy(route_hbm, route_ref, own_sem.at[0]),
           pltpu.make_async_copy(share_hbm, share_ref, own_sem.at[1])]
    own += [
        pltpu.make_async_copy(
            proj_hbm.at[:, pl.ds(q * wcols, wcols)], wbuf.at[q, me], own_sem.at[2 + q]
        )
        for q in range(m)
    ]
    own += [
        pltpu.make_async_copy(ref.at[:, my_cols(me)], buf.at[row_block(me), :], own_sem.at[2 + m + t])
        for t, (ref, buf) in enumerate(trio)
    ]
    loads = [
        pltpu.make_async_copy(res_hbm, res_ref, load_sem.at[3]),
        pltpu.make_async_copy(gain_hbm, gain_ref, load_sem.at[4]),
        pltpu.make_async_copy(gate_hbm.at[0], gate_ref, load_sem.at[0]),
        pltpu.make_async_copy(up_hbm.at[0], up_ref, load_sem.at[1]),
        pltpu.make_async_copy(down_hbm.at[0], down_ref, load_sem.at[2]),
    ]
    for copy in own:
        copy.start()

    relayed = nz == 4
    span = n // 2 if relayed else n
    edge = jnp.logical_or(z == 0, z == nz - 1)
    inner = jnp.logical_not(edge) if relayed else me >= 0
    mate = lax.rem(me + n // 2, n)
    lumps = raw_sem.shape[1]
    lump = width // lumps
    info_copy = pltpu.make_async_remote_copy(
        src_ref=info, dst_ref=mate_info, send_sem=info_sem.at[0], recv_sem=info_sem.at[1],
        device_id=peer(mate, dp), device_id_type=MESH,
    )

    def raw_copy(i):
        part = slice(i * lump, (i + 1) * lump)
        return pltpu.make_async_remote_copy(
            src_ref=normed_ref.at[:, part], dst_ref=raw_ref.at[:, part],
            send_sem=raw_sem.at[0, i], recv_sem=raw_sem.at[1, i],
            device_id=peer(mate, dp), device_id_type=MESH,
        )

    barrier = pltpu.get_barrier_semaphore()
    for off in range(1, n):
        pl.semaphore_signal(barrier, inc=1, device_id=peer(lax.rem(me + off, n), dp), device_id_type=MESH)
    for off in range(1, m):
        pl.semaphore_signal(barrier, inc=1, device_id=peer(me, lax.rem(dp + off, m)), device_id_type=MESH)
    pl.semaphore_wait(barrier, n - 1 + m - 1)

    def in_copy(t, off):
        ref, buf = trio[t]
        to = lax.rem(me + off, n)
        return pltpu.make_async_remote_copy(
            src_ref=ref.at[:, my_cols(to)], dst_ref=buf.at[row_block(me), :],
            send_sem=in_send.at[t, off], recv_sem=in_recv.at[t, me],
            device_id=peer(to, dp), device_id_type=MESH,
        )

    def in_start(t):
        for off in range(1, n):
            in_copy(t, off).start()

    def in_wait(t, origin):
        ref, buf = trio[t]

        @pl.when(me != origin)
        def _():
            pltpu.make_async_remote_copy(
                src_ref=ref.at[:, my_cols(0)], dst_ref=buf.at[row_block(origin), :],
                send_sem=in_send.at[t, 0], recv_sem=in_recv.at[t, origin],
                device_id=peer(origin, dp), device_id_type=MESH,
            ).wait_recv()

    sent = []

    def w_start(cond, q, i, dev, own=False):
        slot = len(sent)
        source = proj_hbm.at[:, pl.ds(pl.multiple_of(q * wcols, wcols), wcols)] if own else wbuf.at[q, i]
        copy = pltpu.make_async_remote_copy(
            src_ref=source, dst_ref=wbuf.at[q, i],
            send_sem=w_send.at[slot], recv_sem=w_recv.at[q, i],
            device_id=dev, device_id_type=MESH,
        )
        sent.append((cond, copy))
        if cond is None:
            copy.start()
        else:
            pl.when(cond)(copy.start)

    def w_wait(cond, q, i):
        copy = pltpu.make_async_remote_copy(
            src_ref=wbuf.at[q, i], dst_ref=wbuf.at[q, i],
            send_sem=w_send.at[0], recv_sem=w_recv.at[q, i],
            device_id=peer(me, lax.rem(dp + 1, m)), device_id_type=MESH,
        )
        if cond is None:
            copy.wait_recv()
        else:
            pl.when(cond)(copy.wait_recv)

    up, down = z + 1 < nz, z > 0
    above, below = jnp.minimum(z + 1, nz - 1) * ny + y, jnp.maximum(z - 1, 0) * ny + y
    other = x * cores + lax.rem(core + 1, cores)

    def across(cond, i):
        for o in range(1, nx):
            w_start(cond, dp, i, peer(me, lax.rem(x + o, nx) * cores + core), False)
        w_start(cond, dp, i, peer(me, other), False)

    def column(dz, upward):
        far = z - dz if upward else z + dz
        cond = far >= 0 if upward else far < nz
        far = jnp.clip(far, 0, nz - 1)
        i = far * ny + y
        w_wait(cond, dp, i)
        more = jnp.logical_and(cond, up if upward else down)
        if dz < nz - 1:
            w_start(more, dp, i, peer(above if upward else below, dp))
        for o in range(1, ny):
            w_start(cond, dp, i, peer(z * ny + lax.rem(y + o, ny), dp))
        across(cond, i)

    def side(dz, upward, o):
        far = z - dz if upward else z + dz
        cond = (far >= 0 if upward else far < nz) if dz else None
        far = jnp.clip(far, 0, nz - 1)
        i = far * ny + lax.rem(y + o, ny)
        w_wait(cond, dp, i)
        across(cond, i)

    def beyond(off, o):
        i = lax.rem(me + off, n)
        q = lax.rem(x + o, nx) * cores + core
        w_wait(None, q, i)
        w_start(None, q, i, peer(me, other))

    def columns(dz):
        column(dz, True)
        column(dz, False)

    def sides(dz):
        for o in range(1, ny):
            side(dz, True, o)
            if dz:
                side(dz, False, o)

    w_start(up, dp, me, peer(above, dp), True)
    w_start(down, dp, me, peer(below, dp), True)
    for o in range(1, ny):
        w_start(None, dp, me, peer(z * ny + lax.rem(y + o, ny), dp), True)
    for load in loads:
        load.start()

    own[0].wait()
    own[1].wait()
    row_id = lax.broadcasted_iota(jnp.int32, (rows, rows), 0)
    col_id = lax.broadcasted_iota(jnp.int32, (rows, rows), 1)
    expert_id = lax.broadcasted_iota(jnp.int32, (n, rows), 0)
    named = [(route_ref[k : k + 1, :] == expert_id).astype(f32) for k in range(2)]
    before = jnp.dot(
        (named[0] + named[1]).astype(bf16), (row_id < col_id).astype(bf16), preferred_element_type=f32
    )
    facts = [
        route_ref[k : k + 1, :].astype(f32) * capacity + jnp.sum(named[k] * before, axis=0, keepdims=True)
        for k in range(2)
    ] + [share_ref[0:1, :], share_ref[1:2, :]]
    for k in range(4):
        info[k : k + 1, :] = facts[k]
    info[4:8, :] = jnp.zeros((4, rows), f32)
    spread = jnp.zeros((rows, rows), f32)
    for k in range(4):
        spread = jnp.where(row_id == k, facts[k], spread)
    cols_ref[...] = spread.T
    if relayed:
        pl.when(edge)(info_copy.start)

    sides(0)
    columns(1)
    sides(1)
    if nz > 2:
        columns(2)
    in_start(0)
    in_start(1)
    if nz > 2:
        sides(2)
    for dz in range(3, nz):
        columns(dz)
    in_start(2)
    for dz in range(3, nz):
        sides(dz)

    scale = math.log2(math.e) / math.sqrt(head)
    later = (row_id > col_id).astype(bf16)
    half = jnp.concatenate([later, jnp.ones((rows, rows), bf16)], axis=1)
    summing = jnp.concatenate([half, half], axis=0)
    log2e = math.log2(math.e)
    chunk = 2 * rows

    for copy in own[2:]:
        copy.wait()

    def weigh(b):
        for h in range(heads_here):
            lanes = slice(h * head, (h + 1) * head)
            key = kbuf[b * rows : (b + 1) * rows, lanes]
            for start in range(b * rows, n * rows, chunk):
                stop = min(start + chunk, n * rows)
                score = lax.dot_general(
                    qbuf[start:stop, lanes], key, (((1,), (1,)), ((), ())), preferred_element_type=f32
                ) * scale
                tail = jnp.log(1.0 + jnp.exp2(-jnp.abs(score))) * log2e
                soft = jnp.maximum(score, 0.0) + tail
                log_sigmoid = jnp.minimum(score, 0.0) - tail
                if start == b * rows:
                    inside = lax.broadcasted_iota(jnp.int32, soft.shape, 1) < lax.broadcasted_iota(
                        jnp.int32, soft.shape, 0
                    )
                    soft = jnp.where(inside, soft, 0.0)
                high = soft.astype(bf16)
                low = (soft - high.astype(f32)).astype(bf16)
                sums = jnp.dot(jnp.concatenate([high, low], axis=1), summing, preferred_element_type=f32)
                part = log_sigmoid - sums[:, :rows]
                fresh = rows if start == b * rows else 0
                if fresh < stop - start:
                    carry = carry_ref[h, start + fresh : stop, :]
                    if fresh:
                        carry = jnp.concatenate([jnp.zeros((fresh, rows), f32), carry], axis=0)
                    part = part - carry
                    total = sums[:, rows:] + carry
                else:
                    total = sums[:, rows:]
                weight = jnp.exp2(part)
                if start == b * rows:
                    weight = jnp.where(inside, weight, 0.0)
                weight_ref[h, start:stop, b * rows : (b + 1) * rows] = weight.astype(bf16)
                if b > 0:
                    carry_ref[h, start:stop, :] = total

    for b in range(n - 1, -1, -1):
        in_wait(0, b)
        in_wait(1, b)
        weigh(b)
    def o_copy(d):
        return pltpu.make_async_remote_copy(
            src_ref=osend.at[d], dst_ref=obuf.at[me],
            send_sem=o_send.at[d], recv_sem=o_recv.at[me],
            device_id=peer(d, dp), device_id_type=MESH,
        )

    for d in range(n):
        in_wait(2, d)
        for h in range(heads_here):
            lanes = slice(h * head, (h + 1) * head)
            osend[d, :, lanes] = jnp.dot(
                weight_ref[h, d * rows : (d + 1) * rows, : (d + 1) * rows],
                vbuf[: (d + 1) * rows, lanes],
                preferred_element_type=f32,
            ).astype(bf16)

        @pl.when(me == d)
        def _():
            obuf[me] = osend[d]

        @pl.when(me != d)
        def _():
            o_copy(d).start()

    for off in range(1, n):
        for o in range(1, nx):
            beyond(off, o)
    for off in range(1, n):
        i = lax.rem(me + off, n)
        for x_off in range(nx):
            w_wait(None, lax.rem(x + x_off, nx) * cores + lax.rem(core + 1, cores), i)
    for load in loads:
        load.wait()

    acc[...] = res_ref[...].astype(f32)

    @pl.loop(0, n)
    def _(step):
        origin = flipped(me, step, n)

        @pl.when(step > 0)
        def _():
            pltpu.make_async_remote_copy(
                src_ref=osend.at[0], dst_ref=obuf.at[origin],
                send_sem=o_send.at[0], recv_sem=o_recv.at[origin],
                device_id=peer(origin, dp), device_id_type=MESH,
            ).wait_recv()

        block = obuf[origin]
        for q in range(m):
            part = slice(q * wcols, (q + 1) * wcols)
            acc[:, part] += jnp.dot(block, wbuf[q, origin], preferred_element_type=f32)

    square = jnp.zeros((rows, 1), f32)
    for q in range(m):
        part = slice(q * wcols, (q + 1) * wcols)
        stream = acc[:, part].astype(bf16)
        stream_ref[:, part] = stream
        stream = stream.astype(f32)
        acc[:, part] = stream
        square = square + jnp.sum(stream * stream, axis=1, keepdims=True)
    factor = lax.rsqrt(square / width + EPS)
    for q in range(m):
        part = slice(q * wcols, (q + 1) * wcols)
        normed_ref[:, part] = (acc[:, part] * factor * gain_ref[:, part]).astype(bf16)

    def chosen(facts, expert):
        slot = lax.broadcasted_iota(jnp.int32, (capacity, rows), 0) + expert * capacity
        slot = slot.astype(f32)
        return jnp.logical_or(facts[0:1, :] == slot, facts[1:2, :] == slot).astype(bf16)

    def there(off):
        return pltpu.make_async_remote_copy(
            src_ref=outgoing.at[off], dst_ref=inbox.at[off],
            send_sem=there_send.at[off], recv_sem=there_recv.at[off],
            device_id=peer(flipped(me, off, n), dp), device_id_type=MESH,
        )

    def relay(off, i):
        part = slice(i * lump, (i + 1) * lump)
        return pltpu.make_async_remote_copy(
            src_ref=relay_out.at[off, :, part], dst_ref=inbox.at[off + span, :, part],
            send_sem=relay_send.at[i, off], recv_sem=there_recv.at[off + span],
            device_id=peer(flipped(me, off, n), dp), device_id_type=MESH,
        )

    def home(off):
        return pltpu.make_async_remote_copy(
            src_ref=outbox.at[off], dst_ref=back.at[off],
            send_sem=back_send.at[off], recv_sem=back_recv.at[off],
            device_id=peer(flipped(me, off, n), dp), device_id_type=MESH,
        )

    def via(off):
        return pltpu.make_async_remote_copy(
            src_ref=outbox.at[off], dst_ref=relay_in.at[off - span],
            send_sem=back_send.at[off], recv_sem=via_recv.at[off - span],
            device_id=peer(flipped(me, off - span, n), dp), device_id_type=MESH,
        )

    def part_copy(i):
        part = slice(i * piece, (i + 1) * piece)
        return pltpu.make_async_remote_copy(
            src_ref=partial_ref.at[:, part], dst_ref=part_ref.at[:, part],
            send_sem=part_sem.at[0, i], recv_sem=part_sem.at[1, i],
            device_id=peer(mate, dp), device_id_type=MESH,
        )

    hidden_width = gate_ref.shape[1]
    piece = width // part_sem.shape[1]
    hidden_piece = min(512, hidden_width)

    if relayed:
        @pl.when(edge)
        def _():
            for i in range(lumps):
                raw_copy(i).start()

    @pl.loop(1, n)
    def _(off):
        @pl.when(jnp.logical_or(inner, off < span))
        def _():
            outgoing[off] = jnp.dot(
                chosen(info, flipped(me, off, n)), normed_ref[...], preferred_element_type=f32
            ).astype(bf16)
            there(off).start()

    inbox[0] = jnp.dot(chosen(info, me), normed_ref[...], preferred_element_type=f32).astype(bf16)

    @pl.loop(0, pairs)
    def _(pair):
        even, odd = pair * 2, pair * 2 + 1
        local = even == 0
        if relayed:
            local = jnp.logical_or(local, jnp.logical_and(inner, even == span))

            @pl.when(jnp.logical_and(inner, even == span))
            def _():
                pltpu.make_async_remote_copy(
                    src_ref=info, dst_ref=mate_info, send_sem=info_sem.at[0], recv_sem=info_sem.at[1],
                    device_id=peer(mate, dp), device_id_type=MESH,
                ).wait_recv()
                for i in range(lumps):
                    part = slice(i * lump, (i + 1) * lump)
                    raw_copy(i).wait_recv()
                    inbox[span, :, part] = jnp.dot(
                        chosen(mate_info, me), raw_ref[:, part], preferred_element_type=f32
                    ).astype(bf16)

                    @pl.loop(1, span)
                    def _(off):
                        relay_out[off, :, part] = jnp.dot(
                            chosen(mate_info, flipped(me, off, n)), raw_ref[:, part],
                            preferred_element_type=f32,
                        ).astype(bf16)
                        relay(off, i).start()

        @pl.when(jnp.logical_not(local))
        def _():
            there(even).wait_recv()

        there(odd).wait_recv()
        arrived = inbox[pl.ds(even, 2)].reshape(2 * capacity, width)
        hidden = []
        for first in range(0, hidden_width, hidden_piece):
            part = slice(first, first + hidden_piece)
            gate = jnp.dot(arrived, gate_ref[:, part], preferred_element_type=f32)
            upper = jnp.dot(arrived, up_ref[:, part], preferred_element_type=f32)
            hidden.append((jax.nn.silu(gate) * upper).astype(bf16))
        hidden = jnp.concatenate(hidden, axis=1)
        for first in range(0, width, piece):
            part = slice(first, first + piece)
            result = jnp.dot(hidden, down_ref[:, part], preferred_element_type=f32)
            outbox[pl.ds(even, 2), :, part] = result.astype(bf16).reshape(2, capacity, piece)

        if relayed:
            side_of = even // ny
            through = side_of == jnp.where(inner, 2, 3)
        else:
            through = even < 0
        direct = jnp.logical_not(through)

        @pl.when(even == 0)
        def _():
            back[0] = outbox[0]

        @pl.when(jnp.logical_and(direct, even > 0))
        def _():
            home(even).start()

        @pl.when(direct)
        def _():
            home(odd).start()

        if relayed:
            @pl.when(jnp.logical_and(through, local))
            def _():
                relay_in[0] = outbox[span]

            @pl.when(jnp.logical_and(through, jnp.logical_not(local)))
            def _():
                via(even).start()

            @pl.when(through)
            def _():
                via(odd).start()

    def picks(facts, even, odd):
        slot = lax.broadcasted_iota(jnp.int32, (rows, 2 * capacity), 1)
        slot = jnp.where(slot < capacity, slot + even * capacity, slot - capacity + odd * capacity)
        slot = slot.astype(f32)
        return [(facts[:, k : k + 1] == slot).astype(bf16) for k in range(2)]

    def shared(facts, pick, block):
        first, second = [jnp.dot(pick[k], block, preferred_element_type=f32) for k in range(2)]
        return facts[:, 2:3] * first + facts[:, 3:4] * second

    def combine(pair):
        @pl.when(pair > 0)
        def _():
            home(pair * 2).wait_recv()

        home(pair * 2 + 1).wait_recv()
        pick = picks(cols_ref, flipped(me, pair * 2, n), flipped(me, pair * 2 + 1, n))
        for start in range(0, width, piece):
            part = slice(start, start + piece)
            block = back[pl.ds(pair * 2, 2), :, part].reshape(2 * capacity, piece)
            acc[:, part] += shared(cols_ref, pick, block)

    @pl.loop(0, span // 2)
    def _(pair):
        combine(pair)

    if relayed:
        @pl.when(inner)
        def _():
            spread = jnp.zeros((rows, rows), f32)
            for k in range(4):
                spread = jnp.where(row_id == k, mate_info[k : k + 1, :], spread)
            mate_cols[...] = spread.T

            @pl.loop(1, span)
            def _(off):
                pltpu.make_async_remote_copy(
                    src_ref=outbox.at[0], dst_ref=relay_in.at[off],
                    send_sem=back_send.at[0], recv_sem=via_recv.at[off],
                    device_id=peer(flipped(me, off, n), dp), device_id_type=MESH,
                ).wait_recv()

            pick = [picks(mate_cols, flipped(me, p * 2, n), flipped(me, p * 2 + 1, n)) for p in range(span // 2)]
            for i in range(width // piece):
                part = slice(i * piece, (i + 1) * piece)
                total = jnp.zeros((rows, piece), f32)
                for p in range(span // 2):
                    block = relay_in[p * 2 : p * 2 + 2, :, part].reshape(2 * capacity, piece)
                    total = total + shared(mate_cols, pick[p], block)
                partial_ref[:, part] = total.astype(bf16)
                part_copy(i).start()

            @pl.loop(span // 2, pairs)
            def _(pair):
                combine(pair)

        @pl.when(edge)
        def _():
            for i in range(width // piece):
                part = slice(i * piece, (i + 1) * piece)
                part_copy(i).wait_recv()
                acc[:, part] += part_ref[:, part].astype(f32)

    out_ref[...] = acc[...].astype(bf16)

    for t in range(3):
        for off in range(1, n):
            in_copy(t, off).wait_send()
    for d in range(n):
        @pl.when(me != d)
        def _():
            o_copy(d).wait_send()
    for cond, copy in sent:
        if cond is None:
            copy.wait_send()
        else:
            pl.when(cond)(copy.wait_send)

    @pl.loop(1, n)
    def _(off):
        @pl.when(jnp.logical_or(inner, off < span))
        def _():
            there(off).wait_send()

        @pl.when(jnp.logical_or(edge, off != span) if relayed else off > 0)
        def _():
            home(off).wait_send()

    if relayed:
        @pl.when(inner)
        def _():
            for i in range(lumps):
                @pl.loop(1, span)
                def _(off):
                    relay(off, i).wait_send()

            for i in range(width // piece):
                part_copy(i).wait_send()

        @pl.when(edge)
        def _():
            info_copy.wait_send()
            for i in range(lumps):
                raw_copy(i).wait_send()


def layer(queries, keys, values, proj_weight, residual, norm_gain, route, share, w_gate, w_up, w_down):
    n, m = lax.axis_size("sp"), lax.axis_size("dp")
    rows, width = queries.shape
    cols = width // n
    ny = 1 << ((n.bit_length() - 1) // 2)
    nz, nx = n // ny, m // 2
    copies = 1 + ny + 2 * nz * (ny + nx + 1) + (2 * nz) * ny * nx + n * nx
    capacity = 4 * rows // n
    hidden = w_gate.shape[2]
    heads_here = cols // (width // HEADS)
    bf16, f32 = jnp.bfloat16, jnp.float32
    return pl.pallas_call(
        functools.partial(layer_kernel, n, m, ny),
        out_shape=jax.ShapeDtypeStruct((rows, width), bf16),
        in_specs=[pl.BlockSpec(memory_space=pl.ANY)] * 11,
        out_specs=pl.BlockSpec(memory_space=pltpu.VMEM),
        scratch_shapes=[
            pltpu.VMEM((n * rows, cols), bf16),
            pltpu.VMEM((n * rows, cols), bf16),
            pltpu.VMEM((n * rows, cols), bf16),
            pltpu.VMEM((m, n, cols, width // m), bf16),
            pltpu.VMEM((n, rows, cols), bf16),
            pltpu.VMEM((n, rows, cols), bf16),
            pltpu.VMEM((heads_here, n * rows, n * rows), bf16),
            pltpu.VMEM((heads_here, n * rows, rows), f32),
            pltpu.VMEM((rows, width), f32),
            pltpu.VMEM((rows, width), bf16),
            pltpu.VMEM((rows, width), bf16),
            pltpu.VMEM((rows, width), bf16),
            pltpu.VMEM((1, width), f32),
            pltpu.VMEM((2, rows), jnp.int32),
            pltpu.VMEM((2, rows), f32),
            pltpu.VMEM((8, rows), f32),
            pltpu.VMEM((rows, rows), f32),
            pltpu.VMEM((width, hidden), bf16),
            pltpu.VMEM((width, hidden), bf16),
            pltpu.VMEM((hidden, width), bf16),
            pltpu.VMEM((n, capacity, width), bf16),
            pltpu.VMEM((n, capacity, width), bf16),
            pltpu.VMEM((n, capacity, width), bf16),
            pltpu.VMEM((n, capacity, width), bf16),
            pltpu.VMEM((rows, width), bf16),
            pltpu.VMEM((n // 2, capacity, width), bf16),
            pltpu.VMEM((n // 2, capacity, width), bf16),
            pltpu.VMEM((rows, width), bf16),
            pltpu.VMEM((rows, width), bf16),
            pltpu.VMEM((8, rows), f32),
            pltpu.VMEM((rows, rows), f32),
            pltpu.SemaphoreType.DMA((5,)),
            pltpu.SemaphoreType.DMA((5 + m,)),
            pltpu.SemaphoreType.DMA((3, n)),
            pltpu.SemaphoreType.DMA((3, n)),
            pltpu.SemaphoreType.DMA((n,)),
            pltpu.SemaphoreType.DMA((n,)),
            pltpu.SemaphoreType.DMA((copies,)),
            pltpu.SemaphoreType.DMA((m, n)),
            pltpu.SemaphoreType.DMA((n,)),
            pltpu.SemaphoreType.DMA((n,)),
            pltpu.SemaphoreType.DMA((n,)),
            pltpu.SemaphoreType.DMA((n,)),
            pltpu.SemaphoreType.DMA((2,)),
            pltpu.SemaphoreType.DMA((2, 2)),
            pltpu.SemaphoreType.DMA((2, n // 2)),
            pltpu.SemaphoreType.DMA((n // 2,)),
            pltpu.SemaphoreType.DMA((2, 4)),
        ],
        compiler_params=pltpu.CompilerParams(
            collective_id=0, has_side_effects=True, vmem_limit_bytes=50 * 1024 * 1024
        ),
    )(
        queries, keys, values, proj_weight, residual, norm_gain.reshape(1, width),
        route.T, share.T, w_gate, w_up, w_down,
    )


def body(
    queries,
    keys,
    values,
    proj_weight,
    residual,
    norm_gain,
    route,
    route_weight,
    w_gate,
    w_up,
    w_down,
):
    return layer(
        queries[0], keys[0], values[0], proj_weight, residual[0], norm_gain,
        route[0], route_weight[0], w_gate, w_up, w_down,
    )[None]


def solution(mesh):
    return jax.shard_map(
        body,
        mesh=mesh,
        in_specs=(
            P("dp", "sp", None),
            P("dp", "sp", None),
            P("dp", "sp", None),
            P("sp", None),
            P("dp", "sp", None),
            P(),
            P("dp", "sp", None),
            P("dp", "sp", None),
            P("sp", None, None),
            P("sp", None, None),
            P("sp", None, None),
        ),
        out_specs=P("dp", "sp", None),
        check_vma=False,
    )
```

```python
import functools
import math

import jax
import jax.numpy as jnp
from jax import lax
from jax.experimental import pallas as pl
from jax.experimental.pallas import tpu as pltpu
from jax.sharding import PartitionSpec as P

HEADS = 16


EPS = 1e-06

MESH = pl.DeviceIdType.MESH


def flipped(number, off, n):
    result = number
    bit = 1
    while bit < n:
        result = result + bit * lax.rem(off // bit, 2) * (1 - 2 * lax.rem(number // bit, 2))
        bit *= 2
    return result


def layer_kernel(
    n, m, ny,
    q_hbm, k_hbm, v_hbm, proj_hbm, res_hbm, gain_hbm, route_hbm, share_hbm, gate_hbm, up_hbm, down_hbm,
    out_ref,
    qbuf, kbuf, vbuf, wbuf, osend, obuf, weight_ref, carry_ref, acc, stream_ref, normed_ref,
    res_ref, gain_ref, route_ref, share_ref, info, cols_ref,
    gate_ref, up_ref, down_ref, outgoing, inbox, outbox, back,
    raw_ref, relay_out, relay_in, partial_ref, part_ref, mate_info, mate_cols,
    load_sem, own_sem,
    in_send, in_recv, o_send, o_recv, w_send, w_recv, there_send, there_recv, back_send, back_recv,
    info_sem, raw_sem, relay_send, via_recv, part_sem,
):
    me, dp = lax.axis_index("sp"), lax.axis_index("dp")
    nz = n // ny
    z, y = me // ny, lax.rem(me, ny)
    cores = 2
    nx = m // cores
    x, core = dp // cores, lax.rem(dp, cores)
    rows, width = stream_ref.shape
    cols = width // n
    head = width // HEADS
    heads_here = cols // head
    wcols = wbuf.shape[3]
    capacity = inbox.shape[1]
    pairs = n // 2
    bf16, f32 = jnp.bfloat16, jnp.float32

    def peer(sp, d):
        return {"sp": sp, "dp": d}

    def my_cols(d):
        return pl.ds(pl.multiple_of(d * cols, cols), cols)

    def row_block(d):
        return pl.ds(pl.multiple_of(d * rows, rows), rows)

    trio = ((k_hbm, kbuf), (q_hbm, qbuf), (v_hbm, vbuf))

    own = [pltpu.make_async_copy(route_hbm, route_ref, own_sem.at[0]),
           pltpu.make_async_copy(share_hbm, share_ref, own_sem.at[1])]
    own += [
        pltpu.make_async_copy(
            proj_hbm.at[:, pl.ds(q * wcols, wcols)], wbuf.at[q, me], own_sem.at[2 + q]
        )
        for q in range(m)
    ]
    own += [
        pltpu.make_async_copy(ref.at[:, my_cols(me)], buf.at[row_block(me), :], own_sem.at[2 + m + t])
        for t, (ref, buf) in enumerate(trio)
    ]
    loads = [
        pltpu.make_async_copy(res_hbm, res_ref, load_sem.at[3]),
        pltpu.make_async_copy(gain_hbm, gain_ref, load_sem.at[4]),
        pltpu.make_async_copy(gate_hbm.at[0], gate_ref, load_sem.at[0]),
        pltpu.make_async_copy(up_hbm.at[0], up_ref, load_sem.at[1]),
        pltpu.make_async_copy(down_hbm.at[0], down_ref, load_sem.at[2]),
    ]
    for copy in own:
        copy.start()

    relayed = nz == 4
    span = n // 2 if relayed else n
    edge = jnp.logical_or(z == 0, z == nz - 1)
    inner = jnp.logical_not(edge) if relayed else me >= 0
    mate = lax.rem(me + n // 2, n)
    lumps = raw_sem.shape[1]
    lump = width // lumps
    info_copy = pltpu.make_async_remote_copy(
        src_ref=info, dst_ref=mate_info, send_sem=info_sem.at[0], recv_sem=info_sem.at[1],
        device_id=peer(mate, dp), device_id_type=MESH,
    )

    def raw_copy(i):
        part = slice(i * lump, (i + 1) * lump)
        return pltpu.make_async_remote_copy(
            src_ref=normed_ref.at[:, part], dst_ref=raw_ref.at[:, part],
            send_sem=raw_sem.at[0, i], recv_sem=raw_sem.at[1, i],
            device_id=peer(mate, dp), device_id_type=MESH,
        )

    barrier = pltpu.get_barrier_semaphore()
    for off in range(1, n):
        pl.semaphore_signal(barrier, inc=1, device_id=peer(lax.rem(me + off, n), dp), device_id_type=MESH)
    for off in range(1, m):
        pl.semaphore_signal(barrier, inc=1, device_id=peer(me, lax.rem(dp + off, m)), device_id_type=MESH)
    pl.semaphore_wait(barrier, n - 1 + m - 1)

    def in_copy(t, off):
        ref, buf = trio[t]
        to = flipped(me, off, n)
        return pltpu.make_async_remote_copy(
            src_ref=ref.at[:, my_cols(to)], dst_ref=buf.at[row_block(me), :],
            send_sem=in_send.at[t, off], recv_sem=in_recv.at[t, me],
            device_id=peer(to, dp), device_id_type=MESH,
        )

    def in_start(t, first=1, last=n):
        for off in range(first, last):
            in_copy(t, off).start()

    def in_wait(t, origin):
        ref, buf = trio[t]

        @pl.when(me != origin)
        def _():
            pltpu.make_async_remote_copy(
                src_ref=ref.at[:, my_cols(0)], dst_ref=buf.at[row_block(origin), :],
                send_sem=in_send.at[t, 0], recv_sem=in_recv.at[t, origin],
                device_id=peer(origin, dp), device_id_type=MESH,
            ).wait_recv()

    sent = []

    def w_start(cond, q, i, dev, own=False):
        slot = len(sent)
        source = proj_hbm.at[:, pl.ds(pl.multiple_of(q * wcols, wcols), wcols)] if own else wbuf.at[q, i]
        copy = pltpu.make_async_remote_copy(
            src_ref=source, dst_ref=wbuf.at[q, i],
            send_sem=w_send.at[slot], recv_sem=w_recv.at[q, i],
            device_id=dev, device_id_type=MESH,
        )
        sent.append((cond, copy))
        if cond is None:
            copy.start()
        else:
            pl.when(cond)(copy.start)

    def w_wait(cond, q, i):
        copy = pltpu.make_async_remote_copy(
            src_ref=wbuf.at[q, i], dst_ref=wbuf.at[q, i],
            send_sem=w_send.at[0], recv_sem=w_recv.at[q, i],
            device_id=peer(me, lax.rem(dp + 1, m)), device_id_type=MESH,
        )
        if cond is None:
            copy.wait_recv()
        else:
            pl.when(cond)(copy.wait_recv)

    up, down = z + 1 < nz, z > 0
    above, below = jnp.minimum(z + 1, nz - 1) * ny + y, jnp.maximum(z - 1, 0) * ny + y
    other = x * cores + lax.rem(core + 1, cores)

    def across(cond, i):
        for o in range(1, nx):
            w_start(cond, dp, i, peer(me, lax.rem(x + o, nx) * cores + core), False)
        w_start(cond, dp, i, peer(me, other), False)

    def column(dz, upward):
        far = z - dz if upward else z + dz
        cond = far >= 0 if upward else far < nz
        far = jnp.clip(far, 0, nz - 1)
        i = far * ny + y
        w_wait(cond, dp, i)
        more = jnp.logical_and(cond, up if upward else down)
        if dz < nz - 1:
            w_start(more, dp, i, peer(above if upward else below, dp))
        for o in range(1, ny):
            w_start(cond, dp, i, peer(z * ny + lax.rem(y + o, ny), dp))
        across(cond, i)

    def side(dz, upward, o):
        far = z - dz if upward else z + dz
        cond = (far >= 0 if upward else far < nz) if dz else None
        far = jnp.clip(far, 0, nz - 1)
        i = far * ny + lax.rem(y + o, ny)
        w_wait(cond, dp, i)
        across(cond, i)

    def beyond(off, o):
        i = lax.rem(me + off, n)
        q = lax.rem(x + o, nx) * cores + core
        w_wait(None, q, i)
        w_start(None, q, i, peer(me, other))

    def columns(dz):
        column(dz, True)
        column(dz, False)

    def sides(dz):
        for o in range(1, ny):
            side(dz, True, o)
            if dz:
                side(dz, False, o)

    w_start(up, dp, me, peer(above, dp), True)
    w_start(down, dp, me, peer(below, dp), True)
    for o in range(1, ny):
        w_start(None, dp, me, peer(z * ny + lax.rem(y + o, ny), dp), True)
    in_start(0, 1, 2 * ny)
    for load in loads:
        load.start()

    own[0].wait()
    own[1].wait()
    row_id = lax.broadcasted_iota(jnp.int32, (rows, rows), 0)
    col_id = lax.broadcasted_iota(jnp.int32, (rows, rows), 1)
    expert_id = lax.broadcasted_iota(jnp.int32, (n, rows), 0)
    named = [(route_ref[k : k + 1, :] == expert_id).astype(f32) for k in range(2)]
    before = jnp.dot(
        (named[0] + named[1]).astype(bf16), (row_id < col_id).astype(bf16), preferred_element_type=f32
    )
    facts = [
        route_ref[k : k + 1, :].astype(f32) * capacity + jnp.sum(named[k] * before, axis=0, keepdims=True)
        for k in range(2)
    ] + [share_ref[0:1, :], share_ref[1:2, :]]
    for k in range(4):
        info[k : k + 1, :] = facts[k]
    info[4:8, :] = jnp.zeros((4, rows), f32)
    spread = jnp.zeros((rows, rows), f32)
    for k in range(4):
        spread = jnp.where(row_id == k, facts[k], spread)
    cols_ref[...] = spread.T
    if relayed:
        pl.when(edge)(info_copy.start)

    columns(1)
    sides(0)
    in_start(0, 2 * ny)
    if nz > 2:
        columns(2)
    in_start(1)
    in_start(2)
    sides(1)
    for dz in range(3, nz):
        columns(dz)

    scale = math.log2(math.e) / math.sqrt(head)
    later = (row_id > col_id).astype(bf16)
    half = jnp.concatenate([later, jnp.ones((rows, rows), bf16)], axis=1)
    summing = jnp.concatenate([half, half], axis=0)
    log2e = math.log2(math.e)
    chunk = 2 * rows

    for copy in own[2:]:
        copy.wait()

    def weigh(b):
        for h in range(heads_here):
            lanes = slice(h * head, (h + 1) * head)
            key = kbuf[b * rows : (b + 1) * rows, lanes]
            for start in range(b * rows, n * rows, chunk):
                stop = min(start + chunk, n * rows)
                score = lax.dot_general(
                    qbuf[start:stop, lanes], key, (((1,), (1,)), ((), ())), preferred_element_type=f32
                ) * scale
                tail = jnp.log(1.0 + jnp.exp2(-jnp.abs(score))) * log2e
                soft = jnp.maximum(score, 0.0) + tail
                log_sigmoid = jnp.minimum(score, 0.0) - tail
                if start == b * rows:
                    inside = lax.broadcasted_iota(jnp.int32, soft.shape, 1) < lax.broadcasted_iota(
                        jnp.int32, soft.shape, 0
                    )
                    soft = jnp.where(inside, soft, 0.0)
                high = soft.astype(bf16)
                low = (soft - high.astype(f32)).astype(bf16)
                sums = jnp.dot(jnp.concatenate([high, low], axis=1), summing, preferred_element_type=f32)
                part = log_sigmoid - sums[:, :rows]
                fresh = rows if start == b * rows else 0
                if fresh < stop - start:
                    carry = carry_ref[h, start + fresh : stop, :]
                    if fresh:
                        carry = jnp.concatenate([jnp.zeros((fresh, rows), f32), carry], axis=0)
                    part = part - carry
                    total = sums[:, rows:] + carry
                else:
                    total = sums[:, rows:]
                weight = jnp.exp2(part)
                if start == b * rows:
                    weight = jnp.where(inside, weight, 0.0)
                weight_ref[h, start:stop, b * rows : (b + 1) * rows] = weight.astype(bf16)
                if b > 0:
                    carry_ref[h, start:stop, :] = total

    for b in range(n - 1, -1, -1):
        in_wait(0, b)
        in_wait(1, b)
        weigh(b)
        if b == n // 2 and nz > 2:
            sides(2)
    for dz in range(3, nz):
        sides(dz)
    def o_copy(d):
        return pltpu.make_async_remote_copy(
            src_ref=osend.at[d], dst_ref=obuf.at[me],
            send_sem=o_send.at[d], recv_sem=o_recv.at[me],
            device_id=peer(d, dp), device_id_type=MESH,
        )

    for d in range(n):
        in_wait(2, d)
        for h in range(heads_here):
            lanes = slice(h * head, (h + 1) * head)
            osend[d, :, lanes] = jnp.dot(
                weight_ref[h, d * rows : (d + 1) * rows, : (d + 1) * rows],
                vbuf[: (d + 1) * rows, lanes],
                preferred_element_type=f32,
            ).astype(bf16)

    obuf[me] = osend[me]

    @pl.loop(1, n)
    def _(off):
        o_copy(flipped(me, off, n)).start()

    for off in range(1, n):
        for o in range(1, nx):
            beyond(off, o)
    for off in range(1, n):
        i = lax.rem(me + off, n)
        for x_off in range(nx):
            w_wait(None, lax.rem(x + x_off, nx) * cores + lax.rem(core + 1, cores), i)
    for load in loads:
        load.wait()

    acc[...] = res_ref[...].astype(f32)

    @pl.loop(0, n)
    def _(step):
        origin = flipped(me, step, n)

        @pl.when(step > 0)
        def _():
            pltpu.make_async_remote_copy(
                src_ref=osend.at[0], dst_ref=obuf.at[origin],
                send_sem=o_send.at[0], recv_sem=o_recv.at[origin],
                device_id=peer(origin, dp), device_id_type=MESH,
            ).wait_recv()

        block = obuf[origin]
        for q in range(m):
            part = slice(q * wcols, (q + 1) * wcols)
            acc[:, part] += jnp.dot(block, wbuf[q, origin], preferred_element_type=f32)

    square = jnp.zeros((rows, 1), f32)
    for q in range(m):
        part = slice(q * wcols, (q + 1) * wcols)
        stream = acc[:, part].astype(bf16)
        stream_ref[:, part] = stream
        stream = stream.astype(f32)
        acc[:, part] = stream
        square = square + jnp.sum(stream * stream, axis=1, keepdims=True)
    factor = lax.rsqrt(square / width + EPS)
    for q in range(m):
        part = slice(q * wcols, (q + 1) * wcols)
        normed_ref[:, part] = (acc[:, part] * factor * gain_ref[:, part]).astype(bf16)

    def chosen(facts, expert):
        slot = lax.broadcasted_iota(jnp.int32, (capacity, rows), 0) + expert * capacity
        slot = slot.astype(f32)
        return jnp.logical_or(facts[0:1, :] == slot, facts[1:2, :] == slot).astype(bf16)

    def there(off):
        return pltpu.make_async_remote_copy(
            src_ref=outgoing.at[off], dst_ref=inbox.at[off],
            send_sem=there_send.at[off], recv_sem=there_recv.at[off],
            device_id=peer(flipped(me, off, n), dp), device_id_type=MESH,
        )

    def relay(off, i):
        part = slice(i * lump, (i + 1) * lump)
        return pltpu.make_async_remote_copy(
            src_ref=relay_out.at[off, :, part], dst_ref=inbox.at[off + span, :, part],
            send_sem=relay_send.at[i, off], recv_sem=there_recv.at[off + span],
            device_id=peer(flipped(me, off, n), dp), device_id_type=MESH,
        )

    def home(off):
        return pltpu.make_async_remote_copy(
            src_ref=outbox.at[off], dst_ref=back.at[off],
            send_sem=back_send.at[off], recv_sem=back_recv.at[off],
            device_id=peer(flipped(me, off, n), dp), device_id_type=MESH,
        )

    def via(off):
        return pltpu.make_async_remote_copy(
            src_ref=outbox.at[off], dst_ref=relay_in.at[off - span],
            send_sem=back_send.at[off], recv_sem=via_recv.at[off - span],
            device_id=peer(flipped(me, off - span, n), dp), device_id_type=MESH,
        )

    def part_copy(i):
        part = slice(i * piece, (i + 1) * piece)
        return pltpu.make_async_remote_copy(
            src_ref=partial_ref.at[:, part], dst_ref=part_ref.at[:, part],
            send_sem=part_sem.at[0, i], recv_sem=part_sem.at[1, i],
            device_id=peer(mate, dp), device_id_type=MESH,
        )

    hidden_width = gate_ref.shape[1]
    piece = width // part_sem.shape[1]
    hidden_piece = min(512, hidden_width)

    if relayed:
        @pl.when(edge)
        def _():
            for i in range(lumps):
                raw_copy(i).start()

    def pack(off):
        outgoing[off] = jnp.dot(
            chosen(info, flipped(me, off, n)), normed_ref[...], preferred_element_type=f32
        ).astype(bf16)

    @pl.loop(1, span)
    def _(off):
        pack(off)
        there(off).start()

    inbox[0] = jnp.dot(chosen(info, me), normed_ref[...], preferred_element_type=f32).astype(bf16)

    if relayed:
        @pl.when(inner)
        def _():
            pl.loop(span, n)(pack)
            info_copy.wait_recv()
            for i in range(lumps):
                part = slice(i * lump, (i + 1) * lump)
                raw_copy(i).wait_recv()

                @pl.loop(1, span)
                def _(off):
                    relay_out[off, :, part] = jnp.dot(
                        chosen(mate_info, flipped(me, off, n)), raw_ref[:, part],
                        preferred_element_type=f32,
                    ).astype(bf16)
                    relay(off, i).start()

                inbox[span, :, part] = jnp.dot(
                    chosen(mate_info, me), raw_ref[:, part], preferred_element_type=f32
                ).astype(bf16)

            @pl.loop(0, span)
            def _(k):
                there(span + lax.rem(k + span // 2, span)).start()

    @pl.loop(0, pairs)
    def _(step):
        pair = step
        if relayed:
            part_of, rest = step // (ny // 2), lax.rem(step, ny // 2)
            middle = jnp.where(part_of == 1, 2, jnp.where(part_of == 2, 1, part_of))
            outer = jnp.where(part_of == 2, 3, jnp.where(part_of == 3, 2, part_of))
            pair = jnp.where(inner, middle, outer) * (ny // 2) + rest
        even, odd = pair * 2, pair * 2 + 1
        local = even == 0
        if relayed:
            local = jnp.logical_or(local, jnp.logical_and(inner, even == span))

        @pl.when(jnp.logical_not(local))
        def _():
            there(even).wait_recv()

        there(odd).wait_recv()
        arrived = inbox[pl.ds(even, 2)].reshape(2 * capacity, width)
        hidden = []
        for first in range(0, hidden_width, hidden_piece):
            part = slice(first, first + hidden_piece)
            gate = jnp.dot(arrived, gate_ref[:, part], preferred_element_type=f32)
            upper = jnp.dot(arrived, up_ref[:, part], preferred_element_type=f32)
            hidden.append((jax.nn.silu(gate) * upper).astype(bf16))
        hidden = jnp.concatenate(hidden, axis=1)
        for first in range(0, width, piece):
            part = slice(first, first + piece)
            result = jnp.dot(hidden, down_ref[:, part], preferred_element_type=f32)
            outbox[pl.ds(even, 2), :, part] = result.astype(bf16).reshape(2, capacity, piece)

        if relayed:
            side_of = even // ny
            through = side_of == jnp.where(inner, 2, 3)
        else:
            through = even < 0
        direct = jnp.logical_not(through)

        @pl.when(even == 0)
        def _():
            back[0] = outbox[0]

        @pl.when(jnp.logical_and(direct, even > 0))
        def _():
            home(even).start()

        @pl.when(direct)
        def _():
            home(odd).start()

        if relayed:
            @pl.when(jnp.logical_and(through, local))
            def _():
                relay_in[0] = outbox[span]

            @pl.when(jnp.logical_and(through, jnp.logical_not(local)))
            def _():
                via(even).start()

            @pl.when(through)
            def _():
                via(odd).start()

    def picks(facts, even, odd):
        slot = lax.broadcasted_iota(jnp.int32, (rows, 2 * capacity), 1)
        slot = jnp.where(slot < capacity, slot + even * capacity, slot - capacity + odd * capacity)
        slot = slot.astype(f32)
        return [(facts[:, k : k + 1] == slot).astype(bf16) for k in range(2)]

    def shared(facts, pick, block):
        first, second = [jnp.dot(pick[k], block, preferred_element_type=f32) for k in range(2)]
        return facts[:, 2:3] * first + facts[:, 3:4] * second

    def combine(pair):
        @pl.when(pair > 0)
        def _():
            home(pair * 2).wait_recv()

        home(pair * 2 + 1).wait_recv()
        pick = picks(cols_ref, flipped(me, pair * 2, n), flipped(me, pair * 2 + 1, n))
        for start in range(0, width, piece):
            part = slice(start, start + piece)
            block = back[pl.ds(pair * 2, 2), :, part].reshape(2 * capacity, piece)
            acc[:, part] += shared(cols_ref, pick, block)

    @pl.loop(0, span // 2)
    def _(pair):
        combine(pair)

    if relayed:
        @pl.when(inner)
        def _():
            spread = jnp.zeros((rows, rows), f32)
            for k in range(4):
                spread = jnp.where(row_id == k, mate_info[k : k + 1, :], spread)
            mate_cols[...] = spread.T

            @pl.loop(1, span)
            def _(off):
                pltpu.make_async_remote_copy(
                    src_ref=outbox.at[0], dst_ref=relay_in.at[off],
                    send_sem=back_send.at[0], recv_sem=via_recv.at[off],
                    device_id=peer(flipped(me, off, n), dp), device_id_type=MESH,
                ).wait_recv()

            pick = [picks(mate_cols, flipped(me, p * 2, n), flipped(me, p * 2 + 1, n)) for p in range(span // 2)]
            for i in range(width // piece):
                part = slice(i * piece, (i + 1) * piece)
                total = jnp.zeros((rows, piece), f32)
                for p in range(span // 2):
                    block = relay_in[p * 2 : p * 2 + 2, :, part].reshape(2 * capacity, piece)
                    total = total + shared(mate_cols, pick[p], block)
                partial_ref[:, part] = total.astype(bf16)
                part_copy(i).start()

            @pl.loop(span // 2, pairs)
            def _(pair):
                combine(pair)

        @pl.when(edge)
        def _():
            for i in range(width // piece):
                part = slice(i * piece, (i + 1) * piece)
                part_copy(i).wait_recv()
                acc[:, part] += part_ref[:, part].astype(f32)

    out_ref[...] = acc[...].astype(bf16)

    for t in range(3):
        for off in range(1, n):
            in_copy(t, off).wait_send()
    @pl.loop(1, n)
    def _(off):
        o_copy(flipped(me, off, n)).wait_send()

    for cond, copy in sent:
        if cond is None:
            copy.wait_send()
        else:
            pl.when(cond)(copy.wait_send)

    @pl.loop(1, n)
    def _(off):
        @pl.when(jnp.logical_or(inner, off < span))
        def _():
            there(off).wait_send()

        @pl.when(jnp.logical_or(edge, off != span) if relayed else off > 0)
        def _():
            home(off).wait_send()

    if relayed:
        @pl.when(inner)
        def _():
            for i in range(lumps):
                @pl.loop(1, span)
                def _(off):
                    relay(off, i).wait_send()

            for i in range(width // piece):
                part_copy(i).wait_send()

        @pl.when(edge)
        def _():
            info_copy.wait_send()
            for i in range(lumps):
                raw_copy(i).wait_send()


def layer(queries, keys, values, proj_weight, residual, norm_gain, route, share, w_gate, w_up, w_down):
    n, m = lax.axis_size("sp"), lax.axis_size("dp")
    rows, width = queries.shape
    cols = width // n
    ny = 1 << ((n.bit_length() - 1) // 2)
    nz, nx = n // ny, m // 2
    copies = 1 + ny + 2 * nz * (ny + nx + 1) + (2 * nz) * ny * nx + n * nx
    capacity = 4 * rows // n
    hidden = w_gate.shape[2]
    heads_here = cols // (width // HEADS)
    bf16, f32 = jnp.bfloat16, jnp.float32
    return pl.pallas_call(
        functools.partial(layer_kernel, n, m, ny),
        out_shape=jax.ShapeDtypeStruct((rows, width), bf16),
        in_specs=[pl.BlockSpec(memory_space=pl.ANY)] * 11,
        out_specs=pl.BlockSpec(memory_space=pltpu.VMEM),
        scratch_shapes=[
            pltpu.VMEM((n * rows, cols), bf16),
            pltpu.VMEM((n * rows, cols), bf16),
            pltpu.VMEM((n * rows, cols), bf16),
            pltpu.VMEM((m, n, cols, width // m), bf16),
            pltpu.VMEM((n, rows, cols), bf16),
            pltpu.VMEM((n, rows, cols), bf16),
            pltpu.VMEM((heads_here, n * rows, n * rows), bf16),
            pltpu.VMEM((heads_here, n * rows, rows), f32),
            pltpu.VMEM((rows, width), f32),
            pltpu.VMEM((rows, width), bf16),
            pltpu.VMEM((rows, width), bf16),
            pltpu.VMEM((rows, width), bf16),
            pltpu.VMEM((1, width), f32),
            pltpu.VMEM((2, rows), jnp.int32),
            pltpu.VMEM((2, rows), f32),
            pltpu.VMEM((8, rows), f32),
            pltpu.VMEM((rows, rows), f32),
            pltpu.VMEM((width, hidden), bf16),
            pltpu.VMEM((width, hidden), bf16),
            pltpu.VMEM((hidden, width), bf16),
            pltpu.VMEM((n, capacity, width), bf16),
            pltpu.VMEM((n, capacity, width), bf16),
            pltpu.VMEM((n, capacity, width), bf16),
            pltpu.VMEM((n, capacity, width), bf16),
            pltpu.VMEM((rows, width), bf16),
            pltpu.VMEM((n // 2, capacity, width), bf16),
            pltpu.VMEM((n // 2, capacity, width), bf16),
            pltpu.VMEM((rows, width), bf16),
            pltpu.VMEM((rows, width), bf16),
            pltpu.VMEM((8, rows), f32),
            pltpu.VMEM((rows, rows), f32),
            pltpu.SemaphoreType.DMA((5,)),
            pltpu.SemaphoreType.DMA((5 + m,)),
            pltpu.SemaphoreType.DMA((3, n)),
            pltpu.SemaphoreType.DMA((3, n)),
            pltpu.SemaphoreType.DMA((n,)),
            pltpu.SemaphoreType.DMA((n,)),
            pltpu.SemaphoreType.DMA((copies,)),
            pltpu.SemaphoreType.DMA((m, n)),
            pltpu.SemaphoreType.DMA((n,)),
            pltpu.SemaphoreType.DMA((n,)),
            pltpu.SemaphoreType.DMA((n,)),
            pltpu.SemaphoreType.DMA((n,)),
            pltpu.SemaphoreType.DMA((2,)),
            pltpu.SemaphoreType.DMA((2, 2)),
            pltpu.SemaphoreType.DMA((2, n // 2)),
            pltpu.SemaphoreType.DMA((n // 2,)),
            pltpu.SemaphoreType.DMA((2, 4)),
        ],
        compiler_params=pltpu.CompilerParams(
            collective_id=0, has_side_effects=True, vmem_limit_bytes=50 * 1024 * 1024
        ),
    )(
        queries, keys, values, proj_weight, residual, norm_gain.reshape(1, width),
        route.T, share.T, w_gate, w_up, w_down,
    )


def body(
    queries,
    keys,
    values,
    proj_weight,
    residual,
    norm_gain,
    route,
    route_weight,
    w_gate,
    w_up,
    w_down,
):
    return layer(
        queries[0], keys[0], values[0], proj_weight, residual[0], norm_gain,
        route[0], route_weight[0], w_gate, w_up, w_down,
    )[None]


def solution(mesh):
    return jax.shard_map(
        body,
        mesh=mesh,
        in_specs=(
            P("dp", "sp", None),
            P("dp", "sp", None),
            P("dp", "sp", None),
            P("sp", None),
            P("dp", "sp", None),
            P(),
            P("dp", "sp", None),
            P("dp", "sp", None),
            P("sp", None, None),
            P("sp", None, None),
            P("sp", None, None),
        ),
        out_specs=P("dp", "sp", None),
        check_vma=False,
    )
```

```python
import functools
import math

import jax
import jax.numpy as jnp
from jax import lax
from jax.experimental import pallas as pl
from jax.experimental.pallas import tpu as pltpu
from jax.sharding import PartitionSpec as P

HEADS = 16


EPS = 1e-06

MESH = pl.DeviceIdType.MESH


def flipped(number, off, n):
    result = number
    bit = 1
    while bit < n:
        result = result + bit * lax.rem(off // bit, 2) * (1 - 2 * lax.rem(number // bit, 2))
        bit *= 2
    return result


def layer_kernel(
    n, m, ny,
    q_hbm, k_hbm, v_hbm, proj_hbm, res_hbm, gain_hbm, route_hbm, share_hbm, gate_hbm, up_hbm, down_hbm,
    out_ref,
    qbuf, kbuf, vbuf, wbuf, osend, obuf, weight_ref, carry_ref, acc, stream_ref, normed_ref,
    res_ref, gain_ref, route_ref, share_ref, info, cols_ref,
    gate_ref, up_ref, down_ref, outgoing, inbox, outbox, back,
    raw_ref, relay_out, relay_in, partial_ref, part_ref, mate_info, mate_cols,
    load_sem, own_sem,
    in_send, in_recv, o_send, o_recv, w_send, w_recv, there_send, there_recv, back_send, back_recv,
    info_send, info_recv, raw_send, raw_recv, relay_send, via_recv, part_send, part_recv,
):
    me, dp = lax.axis_index("sp"), lax.axis_index("dp")
    nz = n // ny
    z, y = me // ny, lax.rem(me, ny)
    cores = 2
    nx = m // cores
    x, core = dp // cores, lax.rem(dp, cores)
    rows, width = stream_ref.shape
    cols = width // n
    head = width // HEADS
    heads_here = cols // head
    wcols = wbuf.shape[3]
    capacity = inbox.shape[1]
    pairs = n // 2
    bf16, f32 = jnp.bfloat16, jnp.float32

    def peer(sp, d):
        return {"sp": sp, "dp": d}

    def my_cols(d):
        return pl.ds(pl.multiple_of(d * cols, cols), cols)

    def row_block(d):
        return pl.ds(pl.multiple_of(d * rows, rows), rows)

    trio = ((k_hbm, kbuf), (q_hbm, qbuf), (v_hbm, vbuf))

    own = [pltpu.make_async_copy(route_hbm, route_ref, own_sem.at[0]),
           pltpu.make_async_copy(share_hbm, share_ref, own_sem.at[1])]
    own += [
        pltpu.make_async_copy(
            proj_hbm.at[:, pl.ds(q * wcols, wcols)], wbuf.at[q, me], own_sem.at[2 + q]
        )
        for q in range(m)
    ]
    own += [
        pltpu.make_async_copy(ref.at[:, my_cols(me)], buf.at[row_block(me), :], own_sem.at[2 + m + t])
        for t, (ref, buf) in enumerate(trio)
    ]
    loads = [
        pltpu.make_async_copy(res_hbm, res_ref, load_sem.at[3]),
        pltpu.make_async_copy(gain_hbm, gain_ref, load_sem.at[4]),
        pltpu.make_async_copy(gate_hbm.at[0], gate_ref, load_sem.at[0]),
        pltpu.make_async_copy(up_hbm.at[0], up_ref, load_sem.at[1]),
        pltpu.make_async_copy(down_hbm.at[0], down_ref, load_sem.at[2]),
    ]
    for copy in own:
        copy.start()

    half = nz // 2
    span = half * ny
    edge = jnp.logical_or(z == 0, z == nz - 1)
    inner = jnp.logical_not(edge)
    slot_of = [half * ny, (nz - 1) * ny]
    my_slot = jnp.where(edge, 0, 1)
    mate = jnp.where(edge, flipped(me, slot_of[0], n), flipped(me, slot_of[1], n))
    lumps = raw_send.shape[0]
    lump = width // lumps

    def info_copy(slot):
        return pltpu.make_async_remote_copy(
            src_ref=info, dst_ref=mate_info.at[slot], send_sem=info_send.at[0], recv_sem=info_recv.at[slot],
            device_id=peer(mate, dp), device_id_type=MESH,
        )

    def raw_copy(slot, i):
        part = slice(i * lump, (i + 1) * lump)
        return pltpu.make_async_remote_copy(
            src_ref=normed_ref.at[:, part], dst_ref=raw_ref.at[slot, :, part],
            send_sem=raw_send.at[i], recv_sem=raw_recv.at[slot, i],
            device_id=peer(mate, dp), device_id_type=MESH,
        )

    barrier = pltpu.get_barrier_semaphore()
    for off in range(1, n):
        pl.semaphore_signal(barrier, inc=1, device_id=peer(lax.rem(me + off, n), dp), device_id_type=MESH)
    for off in range(1, m):
        pl.semaphore_signal(barrier, inc=1, device_id=peer(me, lax.rem(dp + off, m)), device_id_type=MESH)
    pl.semaphore_wait(barrier, n - 1 + m - 1)

    def in_copy(t, off):
        ref, buf = trio[t]
        to = flipped(me, off, n)
        return pltpu.make_async_remote_copy(
            src_ref=ref.at[:, my_cols(to)], dst_ref=buf.at[row_block(me), :],
            send_sem=in_send.at[t, off], recv_sem=in_recv.at[t, me],
            device_id=peer(to, dp), device_id_type=MESH,
        )

    def in_start(t, first=1, last=n):
        for off in range(first, last):
            in_copy(t, off).start()

    def in_wait(t, origin):
        ref, buf = trio[t]

        @pl.when(me != origin)
        def _():
            pltpu.make_async_remote_copy(
                src_ref=ref.at[:, my_cols(0)], dst_ref=buf.at[row_block(origin), :],
                send_sem=in_send.at[t, 0], recv_sem=in_recv.at[t, origin],
                device_id=peer(origin, dp), device_id_type=MESH,
            ).wait_recv()

    sent = []

    def w_start(cond, q, i, dev, own=False):
        slot = len(sent)
        source = proj_hbm.at[:, pl.ds(pl.multiple_of(q * wcols, wcols), wcols)] if own else wbuf.at[q, i]
        copy = pltpu.make_async_remote_copy(
            src_ref=source, dst_ref=wbuf.at[q, i],
            send_sem=w_send.at[slot], recv_sem=w_recv.at[q, i],
            device_id=dev, device_id_type=MESH,
        )
        sent.append((cond, copy))
        if cond is None:
            copy.start()
        else:
            pl.when(cond)(copy.start)

    def w_wait(cond, q, i):
        copy = pltpu.make_async_remote_copy(
            src_ref=wbuf.at[q, i], dst_ref=wbuf.at[q, i],
            send_sem=w_send.at[0], recv_sem=w_recv.at[q, i],
            device_id=peer(me, lax.rem(dp + 1, m)), device_id_type=MESH,
        )
        if cond is None:
            copy.wait_recv()
        else:
            pl.when(cond)(copy.wait_recv)

    up, down = z + 1 < nz, z > 0
    above, below = jnp.minimum(z + 1, nz - 1) * ny + y, jnp.maximum(z - 1, 0) * ny + y
    other = x * cores + lax.rem(core + 1, cores)

    def across(cond, i):
        for o in range(1, nx):
            w_start(cond, dp, i, peer(me, lax.rem(x + o, nx) * cores + core), False)
        w_start(cond, dp, i, peer(me, other), False)

    def column(dz, upward):
        far = z - dz if upward else z + dz
        cond = far >= 0 if upward else far < nz
        far = jnp.clip(far, 0, nz - 1)
        i = far * ny + y
        w_wait(cond, dp, i)
        more = jnp.logical_and(cond, up if upward else down)
        if dz < nz - 1:
            w_start(more, dp, i, peer(above if upward else below, dp))
        for o in range(1, ny):
            w_start(cond, dp, i, peer(z * ny + lax.rem(y + o, ny), dp))
        across(cond, i)

    def side(dz, upward, o):
        far = z - dz if upward else z + dz
        cond = (far >= 0 if upward else far < nz) if dz else None
        far = jnp.clip(far, 0, nz - 1)
        i = far * ny + lax.rem(y + o, ny)
        w_wait(cond, dp, i)
        across(cond, i)

    def beyond(off, o):
        i = lax.rem(me + off, n)
        q = lax.rem(x + o, nx) * cores + core
        w_wait(None, q, i)
        w_start(None, q, i, peer(me, other))

    def columns(dz):
        column(dz, True)
        column(dz, False)

    def sides(dz):
        for o in range(1, ny):
            side(dz, True, o)
            if dz:
                side(dz, False, o)

    w_start(up, dp, me, peer(above, dp), True)
    w_start(down, dp, me, peer(below, dp), True)
    for o in range(1, ny):
        w_start(None, dp, me, peer(z * ny + lax.rem(y + o, ny), dp), True)
    in_start(0, 1, 2 * ny)
    for load in loads:
        load.start()

    own[0].wait()
    own[1].wait()
    row_id = lax.broadcasted_iota(jnp.int32, (rows, rows), 0)
    col_id = lax.broadcasted_iota(jnp.int32, (rows, rows), 1)
    expert_id = lax.broadcasted_iota(jnp.int32, (n, rows), 0)
    named = [(route_ref[k : k + 1, :] == expert_id).astype(f32) for k in range(2)]
    before = jnp.dot(
        (named[0] + named[1]).astype(bf16), (row_id < col_id).astype(bf16), preferred_element_type=f32
    )
    facts = [
        route_ref[k : k + 1, :].astype(f32) * capacity + jnp.sum(named[k] * before, axis=0, keepdims=True)
        for k in range(2)
    ] + [share_ref[0:1, :], share_ref[1:2, :]]
    for k in range(4):
        info[k : k + 1, :] = facts[k]
    info[4:8, :] = jnp.zeros((4, rows), f32)
    spread = jnp.zeros((rows, rows), f32)
    for k in range(4):
        spread = jnp.where(row_id == k, facts[k], spread)
    cols_ref[...] = spread.T
    info_copy(my_slot).start()

    columns(1)
    sides(0)
    in_start(0, 2 * ny)
    if nz > 2:
        columns(2)
    in_start(1)
    in_start(2)
    sides(1)
    for dz in range(3, nz):
        columns(dz)

    scale = math.log2(math.e) / math.sqrt(head)
    later = (row_id > col_id).astype(bf16)
    later_all = jnp.concatenate([later, jnp.ones((rows, rows), bf16)], axis=1)
    summing = jnp.concatenate([later_all, later_all], axis=0)
    log2e = math.log2(math.e)
    chunk = 2 * rows

    for copy in own[2:]:
        copy.wait()

    def weigh(b):
        for h in range(heads_here):
            lanes = slice(h * head, (h + 1) * head)
            key = kbuf[b * rows : (b + 1) * rows, lanes]
            for start in range(b * rows, n * rows, chunk):
                stop = min(start + chunk, n * rows)
                score = lax.dot_general(
                    qbuf[start:stop, lanes], key, (((1,), (1,)), ((), ())), preferred_element_type=f32
                ) * scale
                tail = jnp.log(1.0 + jnp.exp2(-jnp.abs(score))) * log2e
                soft = jnp.maximum(score, 0.0) + tail
                log_sigmoid = jnp.minimum(score, 0.0) - tail
                if start == b * rows:
                    inside = lax.broadcasted_iota(jnp.int32, soft.shape, 1) < lax.broadcasted_iota(
                        jnp.int32, soft.shape, 0
                    )
                    soft = jnp.where(inside, soft, 0.0)
                high = soft.astype(bf16)
                low = (soft - high.astype(f32)).astype(bf16)
                sums = jnp.dot(jnp.concatenate([high, low], axis=1), summing, preferred_element_type=f32)
                part = log_sigmoid - sums[:, :rows]
                fresh = rows if start == b * rows else 0
                if fresh < stop - start:
                    carry = carry_ref[h, start + fresh : stop, :]
                    if fresh:
                        carry = jnp.concatenate([jnp.zeros((fresh, rows), f32), carry], axis=0)
                    part = part - carry
                    total = sums[:, rows:] + carry
                else:
                    total = sums[:, rows:]
                weight = jnp.exp2(part)
                if start == b * rows:
                    weight = jnp.where(inside, weight, 0.0)
                weight_ref[h, start:stop, b * rows : (b + 1) * rows] = weight.astype(bf16)
                if b > 0:
                    carry_ref[h, start:stop, :] = total

    for b in range(n - 1, -1, -1):
        in_wait(0, b)
        in_wait(1, b)
        weigh(b)
        if b == n // 2 and nz > 2:
            sides(2)
    for dz in range(3, nz):
        sides(dz)
    def o_copy(d):
        return pltpu.make_async_remote_copy(
            src_ref=osend.at[d], dst_ref=obuf.at[me],
            send_sem=o_send.at[d], recv_sem=o_recv.at[me],
            device_id=peer(d, dp), device_id_type=MESH,
        )

    for d in range(n):
        in_wait(2, d)
        for h in range(heads_here):
            lanes = slice(h * head, (h + 1) * head)
            osend[d, :, lanes] = jnp.dot(
                weight_ref[h, d * rows : (d + 1) * rows, : (d + 1) * rows],
                vbuf[: (d + 1) * rows, lanes],
                preferred_element_type=f32,
            ).astype(bf16)

    obuf[me] = osend[me]

    @pl.loop(1, n)
    def _(off):
        o_copy(flipped(me, off, n)).start()

    for off in range(1, n):
        for o in range(1, nx):
            beyond(off, o)
    for off in range(1, n):
        i = lax.rem(me + off, n)
        for x_off in range(nx):
            w_wait(None, lax.rem(x + x_off, nx) * cores + lax.rem(core + 1, cores), i)
    for load in loads:
        load.wait()

    acc[...] = res_ref[...].astype(f32)

    @pl.loop(0, n)
    def _(step):
        origin = flipped(me, step, n)

        @pl.when(step > 0)
        def _():
            pltpu.make_async_remote_copy(
                src_ref=osend.at[0], dst_ref=obuf.at[origin],
                send_sem=o_send.at[0], recv_sem=o_recv.at[origin],
                device_id=peer(origin, dp), device_id_type=MESH,
            ).wait_recv()

        block = obuf[origin]
        for q in range(m):
            part = slice(q * wcols, (q + 1) * wcols)
            acc[:, part] += jnp.dot(block, wbuf[q, origin], preferred_element_type=f32)

    square = jnp.zeros((rows, 1), f32)
    for q in range(m):
        part = slice(q * wcols, (q + 1) * wcols)
        stream = acc[:, part].astype(bf16)
        stream_ref[:, part] = stream
        stream = stream.astype(f32)
        acc[:, part] = stream
        square = square + jnp.sum(stream * stream, axis=1, keepdims=True)
    factor = lax.rsqrt(square / width + EPS)
    for q in range(m):
        part = slice(q * wcols, (q + 1) * wcols)
        normed_ref[:, part] = (acc[:, part] * factor * gain_ref[:, part]).astype(bf16)

    def chosen(facts, expert):
        slot = lax.broadcasted_iota(jnp.int32, (capacity, rows), 0) + expert * capacity
        slot = slot.astype(f32)
        return jnp.logical_or(facts[0:1, :] == slot, facts[1:2, :] == slot).astype(bf16)

    def there(off):
        return pltpu.make_async_remote_copy(
            src_ref=outgoing.at[off], dst_ref=inbox.at[off],
            send_sem=there_send.at[off], recv_sem=there_recv.at[off],
            device_id=peer(flipped(me, off, n), dp), device_id_type=MESH,
        )

    def arrival(off):
        return pltpu.make_async_remote_copy(
            src_ref=outgoing.at[0], dst_ref=inbox.at[off],
            send_sem=there_send.at[0], recv_sem=there_recv.at[off],
            device_id=peer(mate, dp), device_id_type=MESH,
        )

    def relay(slot, off, i):
        part = slice(i * lump, (i + 1) * lump)
        index = flipped(off, slot_of[slot], n)
        return pltpu.make_async_remote_copy(
            src_ref=relay_out.at[slot, off, :, part], dst_ref=inbox.at[index, :, part],
            send_sem=relay_send.at[slot, i, off], recv_sem=there_recv.at[index],
            device_id=peer(flipped(me, off, n), dp), device_id_type=MESH,
        )

    def home(off):
        return pltpu.make_async_remote_copy(
            src_ref=outbox.at[off], dst_ref=back.at[off],
            send_sem=back_send.at[off], recv_sem=back_recv.at[off],
            device_id=peer(flipped(me, off, n), dp), device_id_type=MESH,
        )

    hidden_width = gate_ref.shape[1]
    pieces = part_send.shape[1]
    piece = width // pieces
    hidden_piece = min(512, hidden_width)

    def via(off, slot, to, i):
        part = slice(i * piece, (i + 1) * piece)
        return pltpu.make_async_remote_copy(
            src_ref=outbox.at[off, :, part], dst_ref=relay_in.at[slot, to, :, part],
            send_sem=back_send.at[off], recv_sem=via_recv.at[slot, to, i],
            device_id=peer(flipped(me, to, n), dp), device_id_type=MESH,
        )

    def part_copy(slot, i):
        part = slice(i * piece, (i + 1) * piece)
        return pltpu.make_async_remote_copy(
            src_ref=partial_ref.at[slot, :, part], dst_ref=part_ref.at[:, part],
            send_sem=part_send.at[slot, i], recv_sem=part_recv.at[i],
            device_id=peer(flipped(me, slot_of[slot], n), dp), device_id_type=MESH,
        )

    def pack(off):
        outgoing[off] = jnp.dot(
            chosen(info, flipped(me, off, n)), normed_ref[...], preferred_element_type=f32
        ).astype(bf16)
        there(off).start()

    def pass_on(slot, chunks):
        if chunks[0] == 0:
            info_copy(slot).wait_recv()
        for i in chunks:
            part = slice(i * lump, (i + 1) * lump)
            raw_copy(slot, i).wait_recv()

            @pl.loop(1, span)
            def _(step):
                off = span - step
                relay_out[slot, off, :, part] = jnp.dot(
                    chosen(mate_info.at[slot], flipped(me, off, n)), raw_ref[slot, :, part],
                    preferred_element_type=f32,
                ).astype(bf16)
                relay(slot, off, i).start()

            inbox[slot_of[slot], :, part] = jnp.dot(
                chosen(mate_info.at[slot], me), raw_ref[slot, :, part], preferred_element_type=f32
            ).astype(bf16)

    @pl.when(inner)
    def _():
        for i in range(lumps):
            raw_copy(1, i).start()

    pl.loop(1, span)(pack)

    @pl.when(edge)
    def _():
        for i in range(lumps):
            raw_copy(0, i).start()

    inbox[0] = jnp.dot(chosen(info, me), normed_ref[...], preferred_element_type=f32).astype(bf16)

    @pl.when(inner)
    def _():
        pass_on(1, range(1))

    @pl.loop(0, pairs)
    def _(step):
        part_of, rest = step // (ny // 2), lax.rem(step, ny // 2)
        swapped = jnp.where(part_of == 2, 3, jnp.where(part_of == 3, 2, part_of))
        part_of = jnp.where(inner, swapped, part_of)
        even = part_of * ny + rest * 2
        odd = even + 1
        far = part_of >= half
        local = jnp.logical_or(even == 0, jnp.logical_and(inner, jnp.logical_and(far, rest == 0)))

        @pl.when(jnp.logical_and(inner, step == pairs // 4))
        def _():
            pass_on(1, range(1, lumps - 1))

        @pl.when(jnp.logical_and(inner, step == pairs // 2))
        def _():
            pass_on(1, range(lumps - 1, lumps))
            pass_on(0, range(lumps))
            for off in range(ny, span):
                home(off).start()

        @pl.when(jnp.logical_not(local))
        def _():
            arrival(even).wait_recv()

        arrival(odd).wait_recv()
        arrived = inbox[pl.ds(even, 2)].reshape(2 * capacity, width)
        hidden = []
        for first in range(0, hidden_width, hidden_piece):
            part = slice(first, first + hidden_piece)
            gate = jnp.dot(arrived, gate_ref[:, part], preferred_element_type=f32)
            upper = jnp.dot(arrived, up_ref[:, part], preferred_element_type=f32)
            hidden.append((jax.nn.silu(gate) * upper).astype(bf16))
        hidden = jnp.concatenate(hidden, axis=1)
        for first in range(0, width, piece):
            part = slice(first, first + piece)
            result = jnp.dot(hidden, down_ref[:, part], preferred_element_type=f32)
            outbox[pl.ds(even, 2), :, part] = result.astype(bf16).reshape(2, capacity, piece)

        @pl.when(even == 0)
        def _():
            back[0] = outbox[0]

        held = jnp.logical_and(inner, part_of == 1)

        @pl.when(jnp.logical_not(jnp.logical_or(far, held)))
        def _():
            @pl.when(even > 0)
            def _():
                home(even).start()

            home(odd).start()

        @pl.when(far)
        def _():
            slot = jnp.where(inner, part_of - half, nz - 1 - part_of)
            to = jnp.where(inner, 0, ny) + rest * 2

            @pl.when(local)
            def _():
                relay_in[slot, 0] = outbox[even]

            for i in range(pieces):
                @pl.when(jnp.logical_not(local))
                def _():
                    via(even, slot, to, i).start()

                via(odd, slot, to + 1, i).start()

    def picks(facts, even, odd):
        slot = lax.broadcasted_iota(jnp.int32, (rows, 2 * capacity), 1)
        slot = jnp.where(slot < capacity, slot + even * capacity, slot - capacity + odd * capacity)
        slot = slot.astype(f32)
        return [(facts[:, k : k + 1] == slot).astype(bf16) for k in range(2)]

    def shared(facts, pick, block):
        first, second = [jnp.dot(pick[k], block, preferred_element_type=f32) for k in range(2)]
        return facts[:, 2:3] * first + facts[:, 3:4] * second

    @pl.loop(0, span // 2)
    def _(pair):
        @pl.when(pair > 0)
        def _():
            home(pair * 2).wait_recv()

        home(pair * 2 + 1).wait_recv()
        pick = picks(cols_ref, flipped(me, pair * 2, n), flipped(me, pair * 2 + 1, n))
        for start in range(0, width, piece):
            part = slice(start, start + piece)
            block = back[pl.ds(pair * 2, 2), :, part].reshape(2 * capacity, piece)
            acc[:, part] += shared(cols_ref, pick, block)

    @pl.when(inner)
    def _():
        for slot in (1, 0):
            spread = jnp.zeros((rows, rows), f32)
            for k in range(4):
                spread = jnp.where(row_id == k, mate_info[slot, k : k + 1, :], spread)
            mate_cols[slot] = spread.T
            facts = mate_cols.at[slot]
            pick = [picks(facts, flipped(me, p * 2, n), flipped(me, p * 2 + 1, n)) for p in range(span // 2)]
            for i in range(pieces):
                part = slice(i * piece, (i + 1) * piece)

                @pl.loop(1, span)
                def _(to):
                    via(0, slot, to, i).wait_recv()

                total = jnp.zeros((rows, piece), f32)
                for p in range(span // 2):
                    block = relay_in[slot, p * 2 : p * 2 + 2, :, part].reshape(2 * capacity, piece)
                    total = total + shared(facts, pick[p], block)
                partial_ref[slot, :, part] = total.astype(bf16)
                part_copy(slot, i).start()

    for i in range(pieces):
        part = slice(i * piece, (i + 1) * piece)
        part_copy(0, i).wait_recv()
        acc[:, part] += part_ref[:, part].astype(f32)

    out_ref[...] = acc[...].astype(bf16)

    for t in range(3):
        for off in range(1, n):
            in_copy(t, off).wait_send()
    @pl.loop(1, n)
    def _(off):
        o_copy(flipped(me, off, n)).wait_send()

    for cond, copy in sent:
        if cond is None:
            copy.wait_send()
        else:
            pl.when(cond)(copy.wait_send)

    info_copy(my_slot).wait_send()
    for i in range(lumps):
        raw_copy(my_slot, i).wait_send()

    @pl.loop(1, span)
    def _(off):
        there(off).wait_send()

    @pl.loop(1, n)
    def _(off):
        @pl.when(jnp.logical_or(edge, jnp.logical_and(off != slot_of[0], off != slot_of[1])))
        def _():
            pltpu.make_async_remote_copy(
                src_ref=outbox.at[off], dst_ref=inbox.at[off],
                send_sem=back_send.at[off], recv_sem=there_recv.at[off],
                device_id=peer(mate, dp), device_id_type=MESH,
            ).wait_send()

    @pl.when(inner)
    def _():
        for slot in range(2):
            for i in range(lumps):
                @pl.loop(1, span)
                def _(off):
                    relay(slot, off, i).wait_send()

            for i in range(pieces):
                part_copy(slot, i).wait_send()


def layer(queries, keys, values, proj_weight, residual, norm_gain, route, share, w_gate, w_up, w_down):
    n, m = lax.axis_size("sp"), lax.axis_size("dp")
    rows, width = queries.shape
    cols = width // n
    ny = 1 << ((n.bit_length() - 1) // 2)
    nz, nx = n // ny, m // 2
    copies = 1 + ny + 2 * nz * (ny + nx + 1) + (2 * nz) * ny * nx + n * nx
    capacity = 4 * rows // n
    hidden = w_gate.shape[2]
    heads_here = cols // (width // HEADS)
    bf16, f32 = jnp.bfloat16, jnp.float32
    lumps = 4
    return pl.pallas_call(
        functools.partial(layer_kernel, n, m, ny),
        out_shape=jax.ShapeDtypeStruct((rows, width), bf16),
        in_specs=[pl.BlockSpec(memory_space=pl.ANY)] * 11,
        out_specs=pl.BlockSpec(memory_space=pltpu.VMEM),
        scratch_shapes=[
            pltpu.VMEM((n * rows, cols), bf16),
            pltpu.VMEM((n * rows, cols), bf16),
            pltpu.VMEM((n * rows, cols), bf16),
            pltpu.VMEM((m, n, cols, width // m), bf16),
            pltpu.VMEM((n, rows, cols), bf16),
            pltpu.VMEM((n, rows, cols), bf16),
            pltpu.VMEM((heads_here, n * rows, n * rows), bf16),
            pltpu.VMEM((heads_here, n * rows, rows), f32),
            pltpu.VMEM((rows, width), f32),
            pltpu.VMEM((rows, width), bf16),
            pltpu.VMEM((rows, width), bf16),
            pltpu.VMEM((rows, width), bf16),
            pltpu.VMEM((1, width), f32),
            pltpu.VMEM((2, rows), jnp.int32),
            pltpu.VMEM((2, rows), f32),
            pltpu.VMEM((8, rows), f32),
            pltpu.VMEM((rows, rows), f32),
            pltpu.VMEM((width, hidden), bf16),
            pltpu.VMEM((width, hidden), bf16),
            pltpu.VMEM((hidden, width), bf16),
            pltpu.VMEM((n // 2, capacity, width), bf16),
            pltpu.VMEM((n, capacity, width), bf16),
            pltpu.VMEM((n, capacity, width), bf16),
            pltpu.VMEM((n // 2, capacity, width), bf16),
            pltpu.VMEM((2, rows, width), bf16),
            pltpu.VMEM((2, n // 2, capacity, width), bf16),
            pltpu.VMEM((2, n // 2, capacity, width), bf16),
            pltpu.VMEM((2, rows, width), bf16),
            pltpu.VMEM((rows, width), bf16),
            pltpu.VMEM((2, 8, rows), f32),
            pltpu.VMEM((2, rows, rows), f32),
            pltpu.SemaphoreType.DMA((5,)),
            pltpu.SemaphoreType.DMA((5 + m,)),
            pltpu.SemaphoreType.DMA((3, n)),
            pltpu.SemaphoreType.DMA((3, n)),
            pltpu.SemaphoreType.DMA((n,)),
            pltpu.SemaphoreType.DMA((n,)),
            pltpu.SemaphoreType.DMA((copies,)),
            pltpu.SemaphoreType.DMA((m, n)),
            pltpu.SemaphoreType.DMA((n,)),
            pltpu.SemaphoreType.DMA((n,)),
            pltpu.SemaphoreType.DMA((n,)),
            pltpu.SemaphoreType.DMA((n,)),
            pltpu.SemaphoreType.DMA((1,)),
            pltpu.SemaphoreType.DMA((2,)),
            pltpu.SemaphoreType.DMA((lumps,)),
            pltpu.SemaphoreType.DMA((2, lumps)),
            pltpu.SemaphoreType.DMA((2, lumps, n // 2)),
            pltpu.SemaphoreType.DMA((2, n // 2, lumps)),
            pltpu.SemaphoreType.DMA((2, lumps)),
            pltpu.SemaphoreType.DMA((lumps,)),
        ],
        compiler_params=pltpu.CompilerParams(
            collective_id=0, has_side_effects=True, vmem_limit_bytes=50 * 1024 * 1024
        ),
    )(
        queries, keys, values, proj_weight, residual, norm_gain.reshape(1, width),
        route.T, share.T, w_gate, w_up, w_down,
    )


def body(
    queries,
    keys,
    values,
    proj_weight,
    residual,
    norm_gain,
    route,
    route_weight,
    w_gate,
    w_up,
    w_down,
):
    return layer(
        queries[0], keys[0], values[0], proj_weight, residual[0], norm_gain,
        route[0], route_weight[0], w_gate, w_up, w_down,
    )[None]


def solution(mesh):
    return jax.shard_map(
        body,
        mesh=mesh,
        in_specs=(
            P("dp", "sp", None),
            P("dp", "sp", None),
            P("dp", "sp", None),
            P("sp", None),
            P("dp", "sp", None),
            P(),
            P("dp", "sp", None),
            P("dp", "sp", None),
            P("sp", None, None),
            P("sp", None, None),
            P("sp", None, None),
        ),
        out_specs=P("dp", "sp", None),
        check_vma=False,
    )
```

```python
import functools
import math

import jax
import jax.numpy as jnp
from jax import lax
from jax.experimental import pallas as pl
from jax.experimental.pallas import tpu as pltpu
from jax.sharding import PartitionSpec as P

HEADS = 16


EPS = 1e-06

MESH = pl.DeviceIdType.MESH


def flipped(number, off, n):
    result = number
    bit = 1
    while bit < n:
        result = result + bit * lax.rem(off // bit, 2) * (1 - 2 * lax.rem(number // bit, 2))
        bit *= 2
    return result


def layer_kernel(
    n, m, ny,
    q_hbm, k_hbm, v_hbm, proj_hbm, res_hbm, gain_hbm, route_hbm, share_hbm, gate_hbm, up_hbm, down_hbm,
    out_ref,
    qbuf, kbuf, vbuf, wbuf, osend, obuf, weight_ref, carry_ref, acc, stream_ref, normed_ref,
    res_ref, gain_ref, route_ref, share_ref, info, cols_ref,
    gate_ref, up_ref, down_ref, outgoing, inbox, outbox, back,
    raw_ref, relay_out, relay_in, partial_ref, part_ref, mate_info, mate_cols,
    load_sem, own_sem,
    in_send, in_recv, o_send, o_recv, w_send, w_recv, there_send, there_recv, back_send, back_recv,
    info_send, info_recv, raw_send, raw_recv, relay_send, via_recv, part_send, part_recv,
):
    me, dp = lax.axis_index("sp"), lax.axis_index("dp")
    nz = n // ny
    z, y = me // ny, lax.rem(me, ny)
    cores = 2
    nx = m // cores
    x, core = dp // cores, lax.rem(dp, cores)
    rows, width = stream_ref.shape
    cols = width // n
    head = width // HEADS
    heads_here = cols // head
    wcols = wbuf.shape[3]
    capacity = inbox.shape[1]
    pairs = n // 2
    bf16, f32 = jnp.bfloat16, jnp.float32

    def peer(sp, d):
        return {"sp": sp, "dp": d}

    def my_cols(d):
        return pl.ds(pl.multiple_of(d * cols, cols), cols)

    def row_block(d):
        return pl.ds(pl.multiple_of(d * rows, rows), rows)

    trio = ((k_hbm, kbuf), (q_hbm, qbuf), (v_hbm, vbuf))

    own = [pltpu.make_async_copy(route_hbm, route_ref, own_sem.at[0]),
           pltpu.make_async_copy(share_hbm, share_ref, own_sem.at[1])]
    own += [
        pltpu.make_async_copy(
            proj_hbm.at[:, pl.ds(q * wcols, wcols)], wbuf.at[q, me], own_sem.at[2 + q]
        )
        for q in range(m)
    ]
    own += [
        pltpu.make_async_copy(ref.at[:, my_cols(me)], buf.at[row_block(me), :], own_sem.at[2 + m + t])
        for t, (ref, buf) in enumerate(trio)
    ]
    loads = [
        pltpu.make_async_copy(res_hbm, res_ref, load_sem.at[3]),
        pltpu.make_async_copy(gain_hbm, gain_ref, load_sem.at[4]),
        pltpu.make_async_copy(gate_hbm.at[0], gate_ref, load_sem.at[0]),
        pltpu.make_async_copy(up_hbm.at[0], up_ref, load_sem.at[1]),
        pltpu.make_async_copy(down_hbm.at[0], down_ref, load_sem.at[2]),
    ]
    for copy in own:
        copy.start()

    half = nz // 2
    span = half * ny
    edge = jnp.logical_or(z == 0, z == nz - 1)
    inner = jnp.logical_not(edge)
    slot_of = [half * ny, (nz - 1) * ny]
    my_slot = jnp.where(edge, 0, 1)
    mate = jnp.where(edge, flipped(me, slot_of[0], n), flipped(me, slot_of[1], n))
    lumps = raw_send.shape[0]
    lump = width // lumps

    def info_copy(slot):
        return pltpu.make_async_remote_copy(
            src_ref=info, dst_ref=mate_info.at[slot], send_sem=info_send.at[0], recv_sem=info_recv.at[slot],
            device_id=peer(mate, dp), device_id_type=MESH,
        )

    def raw_copy(slot, i):
        part = slice(i * lump, (i + 1) * lump)
        return pltpu.make_async_remote_copy(
            src_ref=normed_ref.at[:, part], dst_ref=raw_ref.at[slot, :, part],
            send_sem=raw_send.at[i], recv_sem=raw_recv.at[slot, i],
            device_id=peer(mate, dp), device_id_type=MESH,
        )

    barrier = pltpu.get_barrier_semaphore()
    for off in range(1, n):
        pl.semaphore_signal(barrier, inc=1, device_id=peer(lax.rem(me + off, n), dp), device_id_type=MESH)
    for off in range(1, m):
        pl.semaphore_signal(barrier, inc=1, device_id=peer(me, lax.rem(dp + off, m)), device_id_type=MESH)
    pl.semaphore_wait(barrier, n - 1 + m - 1)

    def in_copy(t, off):
        ref, buf = trio[t]
        to = flipped(me, off, n)
        return pltpu.make_async_remote_copy(
            src_ref=ref.at[:, my_cols(to)], dst_ref=buf.at[row_block(me), :],
            send_sem=in_send.at[t, off], recv_sem=in_recv.at[t, me],
            device_id=peer(to, dp), device_id_type=MESH,
        )

    def in_start(t, first=1, last=n):
        for off in range(first, last):
            in_copy(t, off).start()

    def in_wait(t, origin):
        ref, buf = trio[t]

        @pl.when(me != origin)
        def _():
            pltpu.make_async_remote_copy(
                src_ref=ref.at[:, my_cols(0)], dst_ref=buf.at[row_block(origin), :],
                send_sem=in_send.at[t, 0], recv_sem=in_recv.at[t, origin],
                device_id=peer(origin, dp), device_id_type=MESH,
            ).wait_recv()

    sent = []

    def w_start(cond, q, i, dev, own=False):
        slot = len(sent)
        source = proj_hbm.at[:, pl.ds(pl.multiple_of(q * wcols, wcols), wcols)] if own else wbuf.at[q, i]
        copy = pltpu.make_async_remote_copy(
            src_ref=source, dst_ref=wbuf.at[q, i],
            send_sem=w_send.at[slot], recv_sem=w_recv.at[q, i],
            device_id=dev, device_id_type=MESH,
        )
        sent.append((cond, copy))
        if cond is None:
            copy.start()
        else:
            pl.when(cond)(copy.start)

    def w_wait(cond, q, i):
        copy = pltpu.make_async_remote_copy(
            src_ref=wbuf.at[q, i], dst_ref=wbuf.at[q, i],
            send_sem=w_send.at[0], recv_sem=w_recv.at[q, i],
            device_id=peer(me, lax.rem(dp + 1, m)), device_id_type=MESH,
        )
        if cond is None:
            copy.wait_recv()
        else:
            pl.when(cond)(copy.wait_recv)

    up, down = z + 1 < nz, z > 0
    above, below = jnp.minimum(z + 1, nz - 1) * ny + y, jnp.maximum(z - 1, 0) * ny + y
    other = x * cores + lax.rem(core + 1, cores)

    def across(cond, i):
        for o in range(1, nx):
            w_start(cond, dp, i, peer(me, lax.rem(x + o, nx) * cores + core), False)
        w_start(cond, dp, i, peer(me, other), False)

    def column(dz, upward):
        far = z - dz if upward else z + dz
        cond = far >= 0 if upward else far < nz
        far = jnp.clip(far, 0, nz - 1)
        i = far * ny + y
        w_wait(cond, dp, i)
        more = jnp.logical_and(cond, up if upward else down)
        if dz < nz - 1:
            w_start(more, dp, i, peer(above if upward else below, dp))
        for o in range(1, ny):
            w_start(cond, dp, i, peer(z * ny + lax.rem(y + o, ny), dp))
        across(cond, i)

    def side(dz, upward, o):
        far = z - dz if upward else z + dz
        cond = (far >= 0 if upward else far < nz) if dz else None
        far = jnp.clip(far, 0, nz - 1)
        i = far * ny + lax.rem(y + o, ny)
        w_wait(cond, dp, i)
        across(cond, i)

    def beyond(off, o):
        i = lax.rem(me + off, n)
        q = lax.rem(x + o, nx) * cores + core
        w_wait(None, q, i)
        w_start(None, q, i, peer(me, other))

    def columns(dz):
        column(dz, True)
        column(dz, False)

    def sides(dz):
        for o in range(1, ny):
            side(dz, True, o)
            if dz:
                side(dz, False, o)

    w_start(up, dp, me, peer(above, dp), True)
    w_start(down, dp, me, peer(below, dp), True)
    for o in range(1, ny):
        w_start(None, dp, me, peer(z * ny + lax.rem(y + o, ny), dp), True)
    in_start(0, 1, 2 * ny)
    for load in loads:
        load.start()

    own[0].wait()
    own[1].wait()
    row_id = lax.broadcasted_iota(jnp.int32, (rows, rows), 0)
    col_id = lax.broadcasted_iota(jnp.int32, (rows, rows), 1)
    expert_id = lax.broadcasted_iota(jnp.int32, (n, rows), 0)
    named = [(route_ref[k : k + 1, :] == expert_id).astype(f32) for k in range(2)]
    before = jnp.dot(
        (named[0] + named[1]).astype(bf16), (row_id < col_id).astype(bf16), preferred_element_type=f32
    )
    facts = [
        route_ref[k : k + 1, :].astype(f32) * capacity + jnp.sum(named[k] * before, axis=0, keepdims=True)
        for k in range(2)
    ] + [share_ref[0:1, :], share_ref[1:2, :]]
    for k in range(4):
        info[k : k + 1, :] = facts[k]
    info[4:8, :] = jnp.zeros((4, rows), f32)
    spread = jnp.zeros((rows, rows), f32)
    for k in range(4):
        spread = jnp.where(row_id == k, facts[k], spread)
    cols_ref[...] = spread.T
    info_copy(my_slot).start()

    columns(1)
    sides(0)
    in_start(0, 2 * ny)
    if nz > 2:
        columns(2)
    in_start(1)
    in_start(2)
    sides(1)
    for dz in range(3, nz):
        columns(dz)

    scale = math.log2(math.e) / math.sqrt(head)
    later = (row_id > col_id).astype(bf16)
    later_all = jnp.concatenate([later, jnp.ones((rows, rows), bf16)], axis=1)
    summing = jnp.concatenate([later_all, later_all], axis=0)
    log2e = math.log2(math.e)
    chunk = 2 * rows

    for copy in own[2:]:
        copy.wait()

    def weigh(b):
        for h in range(heads_here):
            lanes = slice(h * head, (h + 1) * head)
            key = kbuf[b * rows : (b + 1) * rows, lanes]
            for start in range(b * rows, n * rows, chunk):
                stop = min(start + chunk, n * rows)
                score = lax.dot_general(
                    qbuf[start:stop, lanes], key, (((1,), (1,)), ((), ())), preferred_element_type=f32
                ) * scale
                tail = jnp.log(1.0 + jnp.exp2(-jnp.abs(score))) * log2e
                soft = jnp.maximum(score, 0.0) + tail
                log_sigmoid = jnp.minimum(score, 0.0) - tail
                if start == b * rows:
                    inside = lax.broadcasted_iota(jnp.int32, soft.shape, 1) < lax.broadcasted_iota(
                        jnp.int32, soft.shape, 0
                    )
                    soft = jnp.where(inside, soft, 0.0)
                high = soft.astype(bf16)
                low = (soft - high.astype(f32)).astype(bf16)
                sums = jnp.dot(jnp.concatenate([high, low], axis=1), summing, preferred_element_type=f32)
                part = log_sigmoid - sums[:, :rows]
                fresh = rows if start == b * rows else 0
                if fresh < stop - start:
                    carry = carry_ref[h, start + fresh : stop, :]
                    if fresh:
                        carry = jnp.concatenate([jnp.zeros((fresh, rows), f32), carry], axis=0)
                    part = part - carry
                    total = sums[:, rows:] + carry
                else:
                    total = sums[:, rows:]
                weight = jnp.exp2(part)
                if start == b * rows:
                    weight = jnp.where(inside, weight, 0.0)
                weight_ref[h, start:stop, b * rows : (b + 1) * rows] = weight.astype(bf16)
                if b > 0:
                    carry_ref[h, start:stop, :] = total

    for b in range(n - 1, -1, -1):
        in_wait(0, b)
        in_wait(1, b)
        weigh(b)
        if b == n // 2 and nz > 2:
            sides(2)
    for dz in range(3, nz):
        sides(dz)
    def o_copy(d):
        return pltpu.make_async_remote_copy(
            src_ref=osend.at[d], dst_ref=obuf.at[me],
            send_sem=o_send.at[d], recv_sem=o_recv.at[me],
            device_id=peer(d, dp), device_id_type=MESH,
        )

    for d in range(n):
        in_wait(2, d)
        for h in range(heads_here):
            lanes = slice(h * head, (h + 1) * head)
            osend[d, :, lanes] = jnp.dot(
                weight_ref[h, d * rows : (d + 1) * rows, : (d + 1) * rows],
                vbuf[: (d + 1) * rows, lanes],
                preferred_element_type=f32,
            ).astype(bf16)

    obuf[me] = osend[me]

    @pl.loop(1, n)
    def _(off):
        o_copy(flipped(me, n - off, n)).start()

    for off in range(1, n):
        for o in range(1, nx):
            beyond(off, o)
    for off in range(1, n):
        i = lax.rem(me + off, n)
        for x_off in range(nx):
            w_wait(None, lax.rem(x + x_off, nx) * cores + lax.rem(core + 1, cores), i)
    for load in loads:
        load.wait()

    acc[...] = res_ref[...].astype(f32)

    @pl.loop(0, n)
    def _(step):
        origin = flipped(me, step, n)

        @pl.when(step > 0)
        def _():
            pltpu.make_async_remote_copy(
                src_ref=osend.at[0], dst_ref=obuf.at[origin],
                send_sem=o_send.at[0], recv_sem=o_recv.at[origin],
                device_id=peer(origin, dp), device_id_type=MESH,
            ).wait_recv()

        block = obuf[origin]
        for q in range(m):
            part = slice(q * wcols, (q + 1) * wcols)
            acc[:, part] += jnp.dot(block, wbuf[q, origin], preferred_element_type=f32)

    square = jnp.zeros((rows, 1), f32)
    for q in range(m):
        part = slice(q * wcols, (q + 1) * wcols)
        stream = acc[:, part].astype(bf16)
        stream_ref[:, part] = stream
        stream = stream.astype(f32)
        acc[:, part] = stream
        square = square + jnp.sum(stream * stream, axis=1, keepdims=True)
    factor = lax.rsqrt(square / width + EPS)
    for q in range(m):
        part = slice(q * wcols, (q + 1) * wcols)
        normed_ref[:, part] = (acc[:, part] * factor * gain_ref[:, part]).astype(bf16)

    def chosen(facts, expert):
        slot = lax.broadcasted_iota(jnp.int32, (capacity, rows), 0) + expert * capacity
        slot = slot.astype(f32)
        return jnp.logical_or(facts[0:1, :] == slot, facts[1:2, :] == slot).astype(bf16)

    def there(off):
        return pltpu.make_async_remote_copy(
            src_ref=outgoing.at[off], dst_ref=inbox.at[off],
            send_sem=there_send.at[off], recv_sem=there_recv.at[off],
            device_id=peer(flipped(me, off, n), dp), device_id_type=MESH,
        )

    def arrival(off):
        return pltpu.make_async_remote_copy(
            src_ref=outgoing.at[0], dst_ref=inbox.at[off],
            send_sem=there_send.at[0], recv_sem=there_recv.at[off],
            device_id=peer(mate, dp), device_id_type=MESH,
        )

    def relay(slot, off, i):
        part = slice(i * lump, (i + 1) * lump)
        index = flipped(off, slot_of[slot], n)
        return pltpu.make_async_remote_copy(
            src_ref=relay_out.at[slot, off, :, part], dst_ref=inbox.at[index, :, part],
            send_sem=relay_send.at[slot, i, off], recv_sem=there_recv.at[index],
            device_id=peer(flipped(me, off, n), dp), device_id_type=MESH,
        )

    def home(off):
        return pltpu.make_async_remote_copy(
            src_ref=outbox.at[off], dst_ref=back.at[off],
            send_sem=back_send.at[off], recv_sem=back_recv.at[off],
            device_id=peer(flipped(me, off, n), dp), device_id_type=MESH,
        )

    hidden_width = gate_ref.shape[1]
    pieces = part_send.shape[1]
    piece = width // pieces
    hidden_piece = min(512, hidden_width)

    def via(off, slot, to, i):
        part = slice(i * piece, (i + 1) * piece)
        return pltpu.make_async_remote_copy(
            src_ref=outbox.at[off, :, part], dst_ref=relay_in.at[slot, to, :, part],
            send_sem=back_send.at[off], recv_sem=via_recv.at[slot, to, i],
            device_id=peer(flipped(me, to, n), dp), device_id_type=MESH,
        )

    def part_copy(slot, i):
        part = slice(i * piece, (i + 1) * piece)
        return pltpu.make_async_remote_copy(
            src_ref=partial_ref.at[slot, :, part], dst_ref=part_ref.at[:, part],
            send_sem=part_send.at[slot, i], recv_sem=part_recv.at[i],
            device_id=peer(flipped(me, slot_of[slot], n), dp), device_id_type=MESH,
        )

    def pack(off):
        outgoing[off] = jnp.dot(
            chosen(info, flipped(me, off, n)), normed_ref[...], preferred_element_type=f32
        ).astype(bf16)
        there(off).start()

    def pass_on(slot, chunks):
        if chunks[0] == 0:
            info_copy(slot).wait_recv()
        for i in chunks:
            part = slice(i * lump, (i + 1) * lump)
            raw_copy(slot, i).wait_recv()

            @pl.loop(1, span)
            def _(step):
                off = span - step
                relay_out[slot, off, :, part] = jnp.dot(
                    chosen(mate_info.at[slot], flipped(me, off, n)), raw_ref[slot, :, part],
                    preferred_element_type=f32,
                ).astype(bf16)
                relay(slot, off, i).start()

            inbox[slot_of[slot], :, part] = jnp.dot(
                chosen(mate_info.at[slot], me), raw_ref[slot, :, part], preferred_element_type=f32
            ).astype(bf16)

    @pl.when(inner)
    def _():
        for i in range(lumps):
            raw_copy(1, i).start()

    pl.loop(1, span)(pack)

    @pl.when(edge)
    def _():
        for i in range(lumps):
            raw_copy(0, i).start()

    inbox[0] = jnp.dot(chosen(info, me), normed_ref[...], preferred_element_type=f32).astype(bf16)

    @pl.when(inner)
    def _():
        pass_on(1, range(1))

    @pl.loop(0, pairs)
    def _(step):
        part_of, rest = step // (ny // 2), lax.rem(step, ny // 2)
        swapped = jnp.where(part_of == 2, 3, jnp.where(part_of == 3, 2, part_of))
        part_of = jnp.where(inner, swapped, part_of)
        even = part_of * ny + rest * 2
        odd = even + 1
        far = part_of >= half
        local = jnp.logical_or(even == 0, jnp.logical_and(inner, jnp.logical_and(far, rest == 0)))

        @pl.when(jnp.logical_and(inner, step == pairs // 4))
        def _():
            pass_on(1, range(1, lumps - 1))

        @pl.when(jnp.logical_and(inner, step == pairs // 2))
        def _():
            pass_on(1, range(lumps - 1, lumps))
            pass_on(0, range(lumps))
            for off in range(ny, span):
                home(off).start()

        @pl.when(jnp.logical_not(local))
        def _():
            arrival(even).wait_recv()

        arrival(odd).wait_recv()
        arrived = inbox[pl.ds(even, 2)].reshape(2 * capacity, width)
        hidden = []
        for first in range(0, hidden_width, hidden_piece):
            part = slice(first, first + hidden_piece)
            gate = jnp.dot(arrived, gate_ref[:, part], preferred_element_type=f32)
            upper = jnp.dot(arrived, up_ref[:, part], preferred_element_type=f32)
            hidden.append((jax.nn.silu(gate) * upper).astype(bf16))
        hidden = jnp.concatenate(hidden, axis=1)
        for first in range(0, width, piece):
            part = slice(first, first + piece)
            result = jnp.dot(hidden, down_ref[:, part], preferred_element_type=f32)
            outbox[pl.ds(even, 2), :, part] = result.astype(bf16).reshape(2, capacity, piece)

        @pl.when(even == 0)
        def _():
            back[0] = outbox[0]

        held = jnp.logical_and(inner, part_of == 1)

        @pl.when(jnp.logical_not(jnp.logical_or(far, held)))
        def _():
            @pl.when(even > 0)
            def _():
                home(even).start()

            home(odd).start()

        @pl.when(far)
        def _():
            slot = jnp.where(inner, part_of - half, nz - 1 - part_of)
            to = jnp.where(inner, 0, ny) + rest * 2

            @pl.when(local)
            def _():
                relay_in[slot, 0] = outbox[even]

            for i in range(pieces):
                @pl.when(jnp.logical_not(local))
                def _():
                    via(even, slot, to, i).start()

                via(odd, slot, to + 1, i).start()

    def picks(facts, even, odd):
        slot = lax.broadcasted_iota(jnp.int32, (rows, 2 * capacity), 1)
        slot = jnp.where(slot < capacity, slot + even * capacity, slot - capacity + odd * capacity)
        slot = slot.astype(f32)
        return [(facts[:, k : k + 1] == slot).astype(bf16) for k in range(2)]

    def shared(facts, pick, block):
        first, second = [jnp.dot(pick[k], block, preferred_element_type=f32) for k in range(2)]
        return facts[:, 2:3] * first + facts[:, 3:4] * second

    @pl.loop(0, span // 2)
    def _(pair):
        @pl.when(pair > 0)
        def _():
            home(pair * 2).wait_recv()

        home(pair * 2 + 1).wait_recv()
        pick = picks(cols_ref, flipped(me, pair * 2, n), flipped(me, pair * 2 + 1, n))
        for start in range(0, width, piece):
            part = slice(start, start + piece)
            block = back[pl.ds(pair * 2, 2), :, part].reshape(2 * capacity, piece)
            acc[:, part] += shared(cols_ref, pick, block)

    @pl.when(inner)
    def _():
        for slot in (1, 0):
            spread = jnp.zeros((rows, rows), f32)
            for k in range(4):
                spread = jnp.where(row_id == k, mate_info[slot, k : k + 1, :], spread)
            mate_cols[slot] = spread.T
            facts = mate_cols.at[slot]
            pick = [picks(facts, flipped(me, p * 2, n), flipped(me, p * 2 + 1, n)) for p in range(span // 2)]
            for i in range(pieces):
                part = slice(i * piece, (i + 1) * piece)

                @pl.loop(1, span)
                def _(to):
                    via(0, slot, to, i).wait_recv()

                total = jnp.zeros((rows, piece), f32)
                for p in range(span // 2):
                    block = relay_in[slot, p * 2 : p * 2 + 2, :, part].reshape(2 * capacity, piece)
                    total = total + shared(facts, pick[p], block)
                partial_ref[slot, :, part] = total.astype(bf16)
                part_copy(slot, i).start()

    for i in range(pieces):
        part = slice(i * piece, (i + 1) * piece)
        part_copy(0, i).wait_recv()
        acc[:, part] += part_ref[:, part].astype(f32)

    out_ref[...] = acc[...].astype(bf16)

    for t in range(3):
        for off in range(1, n):
            in_copy(t, off).wait_send()
    @pl.loop(1, n)
    def _(off):
        o_copy(flipped(me, off, n)).wait_send()

    for cond, copy in sent:
        if cond is None:
            copy.wait_send()
        else:
            pl.when(cond)(copy.wait_send)

    info_copy(my_slot).wait_send()
    for i in range(lumps):
        raw_copy(my_slot, i).wait_send()

    @pl.loop(1, span)
    def _(off):
        there(off).wait_send()

    @pl.loop(1, n)
    def _(off):
        @pl.when(jnp.logical_or(edge, jnp.logical_and(off != slot_of[0], off != slot_of[1])))
        def _():
            pltpu.make_async_remote_copy(
                src_ref=outbox.at[off], dst_ref=inbox.at[off],
                send_sem=back_send.at[off], recv_sem=there_recv.at[off],
                device_id=peer(mate, dp), device_id_type=MESH,
            ).wait_send()

    @pl.when(inner)
    def _():
        for slot in range(2):
            for i in range(lumps):
                @pl.loop(1, span)
                def _(off):
                    relay(slot, off, i).wait_send()

            for i in range(pieces):
                part_copy(slot, i).wait_send()


def layer(queries, keys, values, proj_weight, residual, norm_gain, route, share, w_gate, w_up, w_down):
    n, m = lax.axis_size("sp"), lax.axis_size("dp")
    rows, width = queries.shape
    cols = width // n
    ny = 1 << ((n.bit_length() - 1) // 2)
    nz, nx = n // ny, m // 2
    copies = 1 + ny + 2 * nz * (ny + nx + 1) + (2 * nz) * ny * nx + n * nx
    capacity = 4 * rows // n
    hidden = w_gate.shape[2]
    heads_here = cols // (width // HEADS)
    bf16, f32 = jnp.bfloat16, jnp.float32
    lumps = 4
    return pl.pallas_call(
        functools.partial(layer_kernel, n, m, ny),
        out_shape=jax.ShapeDtypeStruct((rows, width), bf16),
        in_specs=[pl.BlockSpec(memory_space=pl.ANY)] * 11,
        out_specs=pl.BlockSpec(memory_space=pltpu.VMEM),
        scratch_shapes=[
            pltpu.VMEM((n * rows, cols), bf16),
            pltpu.VMEM((n * rows, cols), bf16),
            pltpu.VMEM((n * rows, cols), bf16),
            pltpu.VMEM((m, n, cols, width // m), bf16),
            pltpu.VMEM((n, rows, cols), bf16),
            pltpu.VMEM((n, rows, cols), bf16),
            pltpu.VMEM((heads_here, n * rows, n * rows), bf16),
            pltpu.VMEM((heads_here, n * rows, rows), f32),
            pltpu.VMEM((rows, width), f32),
            pltpu.VMEM((rows, width), bf16),
            pltpu.VMEM((rows, width), bf16),
            pltpu.VMEM((rows, width), bf16),
            pltpu.VMEM((1, width), f32),
            pltpu.VMEM((2, rows), jnp.int32),
            pltpu.VMEM((2, rows), f32),
            pltpu.VMEM((8, rows), f32),
            pltpu.VMEM((rows, rows), f32),
            pltpu.VMEM((width, hidden), bf16),
            pltpu.VMEM((width, hidden), bf16),
            pltpu.VMEM((hidden, width), bf16),
            pltpu.VMEM((n // 2, capacity, width), bf16),
            pltpu.VMEM((n, capacity, width), bf16),
            pltpu.VMEM((n, capacity, width), bf16),
            pltpu.VMEM((n // 2, capacity, width), bf16),
            pltpu.VMEM((2, rows, width), bf16),
            pltpu.VMEM((2, n // 2, capacity, width), bf16),
            pltpu.VMEM((2, n // 2, capacity, width), bf16),
            pltpu.VMEM((2, rows, width), bf16),
            pltpu.VMEM((rows, width), bf16),
            pltpu.VMEM((2, 8, rows), f32),
            pltpu.VMEM((2, rows, rows), f32),
            pltpu.SemaphoreType.DMA((5,)),
            pltpu.SemaphoreType.DMA((5 + m,)),
            pltpu.SemaphoreType.DMA((3, n)),
            pltpu.SemaphoreType.DMA((3, n)),
            pltpu.SemaphoreType.DMA((n,)),
            pltpu.SemaphoreType.DMA((n,)),
            pltpu.SemaphoreType.DMA((copies,)),
            pltpu.SemaphoreType.DMA((m, n)),
            pltpu.SemaphoreType.DMA((n,)),
            pltpu.SemaphoreType.DMA((n,)),
            pltpu.SemaphoreType.DMA((n,)),
            pltpu.SemaphoreType.DMA((n,)),
            pltpu.SemaphoreType.DMA((1,)),
            pltpu.SemaphoreType.DMA((2,)),
            pltpu.SemaphoreType.DMA((lumps,)),
            pltpu.SemaphoreType.DMA((2, lumps)),
            pltpu.SemaphoreType.DMA((2, lumps, n // 2)),
            pltpu.SemaphoreType.DMA((2, n // 2, lumps)),
            pltpu.SemaphoreType.DMA((2, lumps)),
            pltpu.SemaphoreType.DMA((lumps,)),
        ],
        compiler_params=pltpu.CompilerParams(
            collective_id=0, has_side_effects=True, vmem_limit_bytes=50 * 1024 * 1024
        ),
    )(
        queries, keys, values, proj_weight, residual, norm_gain.reshape(1, width),
        route.T, share.T, w_gate, w_up, w_down,
    )


def body(
    queries,
    keys,
    values,
    proj_weight,
    residual,
    norm_gain,
    route,
    route_weight,
    w_gate,
    w_up,
    w_down,
):
    return layer(
        queries[0], keys[0], values[0], proj_weight, residual[0], norm_gain,
        route[0], route_weight[0], w_gate, w_up, w_down,
    )[None]


def solution(mesh):
    return jax.shard_map(
        body,
        mesh=mesh,
        in_specs=(
            P("dp", "sp", None),
            P("dp", "sp", None),
            P("dp", "sp", None),
            P("sp", None),
            P("dp", "sp", None),
            P(),
            P("dp", "sp", None),
            P("dp", "sp", None),
            P("sp", None, None),
            P("sp", None, None),
            P("sp", None, None),
        ),
        out_specs=P("dp", "sp", None),
        check_vma=False,
    )
```

```python
import functools
import math

import jax
import jax.numpy as jnp
from jax import lax
from jax.experimental import pallas as pl
from jax.experimental.pallas import tpu as pltpu
from jax.sharding import PartitionSpec as P

HEADS = 16


EPS = 1e-06

MESH = pl.DeviceIdType.MESH


def flipped(number, off, n):
    result = number
    bit = 1
    while bit < n:
        result = result + bit * lax.rem(off // bit, 2) * (1 - 2 * lax.rem(number // bit, 2))
        bit *= 2
    return result


def layer_kernel(
    n, m, ny,
    q_hbm, k_hbm, v_hbm, proj_hbm, res_hbm, gain_hbm, route_hbm, share_hbm, gate_hbm, up_hbm, down_hbm,
    out_ref,
    qbuf, kbuf, vbuf, wbuf, osend, obuf, weight_ref, carry_ref, acc, stream_ref, normed_ref,
    res_ref, gain_ref, route_ref, share_ref, info, cols_ref,
    gate_ref, up_ref, down_ref, outgoing, inbox, outbox, back,
    raw_ref, relay_out, relay_in, partial_ref, part_ref, mate_info, mate_cols,
    load_sem, own_sem,
    in_send, in_recv, o_send, o_recv, w_send, w_recv, there_send, there_recv, back_send, back_recv,
    info_send, info_recv, raw_send, raw_recv, relay_send, via_recv, part_send, part_recv,
):
    me, dp = lax.axis_index("sp"), lax.axis_index("dp")
    nz = n // ny
    z, y = me // ny, lax.rem(me, ny)
    cores = 2
    nx = m // cores
    x, core = dp // cores, lax.rem(dp, cores)
    rows, width = stream_ref.shape
    cols = width // n
    head = width // HEADS
    heads_here = cols // head
    wcols = wbuf.shape[3]
    capacity = inbox.shape[1]
    pairs = n // 2
    bf16, f32 = jnp.bfloat16, jnp.float32

    def peer(sp, d):
        return {"sp": sp, "dp": d}

    def my_cols(d):
        return pl.ds(pl.multiple_of(d * cols, cols), cols)

    def row_block(d):
        return pl.ds(pl.multiple_of(d * rows, rows), rows)

    trio = ((k_hbm, kbuf), (q_hbm, qbuf), (v_hbm, vbuf))

    own = [pltpu.make_async_copy(route_hbm, route_ref, own_sem.at[0]),
           pltpu.make_async_copy(share_hbm, share_ref, own_sem.at[1])]
    own += [
        pltpu.make_async_copy(
            proj_hbm.at[:, pl.ds(q * wcols, wcols)], wbuf.at[q, me], own_sem.at[2 + q]
        )
        for q in range(m)
    ]
    own += [
        pltpu.make_async_copy(ref.at[:, my_cols(me)], buf.at[row_block(me), :], own_sem.at[2 + m + t])
        for t, (ref, buf) in enumerate(trio)
    ]
    loads = [
        pltpu.make_async_copy(res_hbm, res_ref, load_sem.at[3]),
        pltpu.make_async_copy(gain_hbm, gain_ref, load_sem.at[4]),
        pltpu.make_async_copy(gate_hbm.at[0], gate_ref, load_sem.at[0]),
        pltpu.make_async_copy(up_hbm.at[0], up_ref, load_sem.at[1]),
        pltpu.make_async_copy(down_hbm.at[0], down_ref, load_sem.at[2]),
    ]
    for copy in own:
        copy.start()

    half = nz // 2
    span = half * ny
    edge = jnp.logical_or(z == 0, z == nz - 1)
    inner = jnp.logical_not(edge)
    slot_of = [half * ny, (nz - 1) * ny]
    my_slot = jnp.where(edge, 0, 1)
    mate = jnp.where(edge, flipped(me, slot_of[0], n), flipped(me, slot_of[1], n))
    lumps = raw_send.shape[0]
    lump = width // lumps

    def info_copy(slot):
        return pltpu.make_async_remote_copy(
            src_ref=info, dst_ref=mate_info.at[slot], send_sem=info_send.at[0], recv_sem=info_recv.at[slot],
            device_id=peer(mate, dp), device_id_type=MESH,
        )

    def raw_copy(slot, i):
        part = slice(i * lump, (i + 1) * lump)
        return pltpu.make_async_remote_copy(
            src_ref=normed_ref.at[:, part], dst_ref=raw_ref.at[slot, :, part],
            send_sem=raw_send.at[i], recv_sem=raw_recv.at[slot, i],
            device_id=peer(mate, dp), device_id_type=MESH,
        )

    barrier = pltpu.get_barrier_semaphore()
    for off in range(1, n):
        pl.semaphore_signal(barrier, inc=1, device_id=peer(lax.rem(me + off, n), dp), device_id_type=MESH)
    for off in range(1, m):
        pl.semaphore_signal(barrier, inc=1, device_id=peer(me, lax.rem(dp + off, m)), device_id_type=MESH)
    pl.semaphore_wait(barrier, n - 1 + m - 1)

    def in_copy(t, off):
        ref, buf = trio[t]
        to = flipped(me, off, n)
        return pltpu.make_async_remote_copy(
            src_ref=ref.at[:, my_cols(to)], dst_ref=buf.at[row_block(me), :],
            send_sem=in_send.at[t, off], recv_sem=in_recv.at[t, me],
            device_id=peer(to, dp), device_id_type=MESH,
        )

    def in_start(t, first=1, last=n):
        for off in range(first, last):
            in_copy(t, off).start()

    def in_wait(t, origin):
        ref, buf = trio[t]

        @pl.when(me != origin)
        def _():
            pltpu.make_async_remote_copy(
                src_ref=ref.at[:, my_cols(0)], dst_ref=buf.at[row_block(origin), :],
                send_sem=in_send.at[t, 0], recv_sem=in_recv.at[t, origin],
                device_id=peer(origin, dp), device_id_type=MESH,
            ).wait_recv()

    sent = []

    def w_start(cond, q, i, dev, own=False):
        slot = len(sent)
        source = proj_hbm.at[:, pl.ds(pl.multiple_of(q * wcols, wcols), wcols)] if own else wbuf.at[q, i]
        copy = pltpu.make_async_remote_copy(
            src_ref=source, dst_ref=wbuf.at[q, i],
            send_sem=w_send.at[slot], recv_sem=w_recv.at[q, i],
            device_id=dev, device_id_type=MESH,
        )
        sent.append((cond, copy))
        if cond is None:
            copy.start()
        else:
            pl.when(cond)(copy.start)

    def w_wait(cond, q, i):
        copy = pltpu.make_async_remote_copy(
            src_ref=wbuf.at[q, i], dst_ref=wbuf.at[q, i],
            send_sem=w_send.at[0], recv_sem=w_recv.at[q, i],
            device_id=peer(me, lax.rem(dp + 1, m)), device_id_type=MESH,
        )
        if cond is None:
            copy.wait_recv()
        else:
            pl.when(cond)(copy.wait_recv)

    up, down = z + 1 < nz, z > 0
    above, below = jnp.minimum(z + 1, nz - 1) * ny + y, jnp.maximum(z - 1, 0) * ny + y
    other = x * cores + lax.rem(core + 1, cores)

    def across(cond, i):
        for o in range(1, nx):
            w_start(cond, dp, i, peer(me, lax.rem(x + o, nx) * cores + core), False)
        w_start(cond, dp, i, peer(me, other), False)

    def column(dz, upward):
        far = z - dz if upward else z + dz
        cond = far >= 0 if upward else far < nz
        far = jnp.clip(far, 0, nz - 1)
        i = far * ny + y
        w_wait(cond, dp, i)
        more = jnp.logical_and(cond, up if upward else down)
        if dz < nz - 1:
            w_start(more, dp, i, peer(above if upward else below, dp))
        for o in range(1, ny):
            w_start(cond, dp, i, peer(z * ny + lax.rem(y + o, ny), dp))
        across(cond, i)

    def side(dz, upward, o):
        far = z - dz if upward else z + dz
        cond = (far >= 0 if upward else far < nz) if dz else None
        far = jnp.clip(far, 0, nz - 1)
        i = far * ny + lax.rem(y + o, ny)
        w_wait(cond, dp, i)
        across(cond, i)

    def beyond(off, o):
        i = lax.rem(me + off, n)
        q = lax.rem(x + o, nx) * cores + core
        w_wait(None, q, i)
        w_start(None, q, i, peer(me, other))

    def columns(dz):
        column(dz, True)
        column(dz, False)

    def sides(dz):
        for o in range(1, ny):
            side(dz, True, o)
            if dz:
                side(dz, False, o)

    w_start(up, dp, me, peer(above, dp), True)
    w_start(down, dp, me, peer(below, dp), True)
    for o in range(1, ny):
        w_start(None, dp, me, peer(z * ny + lax.rem(y + o, ny), dp), True)
    in_start(0, 1, 2 * ny)
    for load in loads:
        load.start()

    own[0].wait()
    own[1].wait()
    row_id = lax.broadcasted_iota(jnp.int32, (rows, rows), 0)
    col_id = lax.broadcasted_iota(jnp.int32, (rows, rows), 1)
    expert_id = lax.broadcasted_iota(jnp.int32, (n, rows), 0)
    named = [(route_ref[k : k + 1, :] == expert_id).astype(f32) for k in range(2)]
    before = jnp.dot(
        (named[0] + named[1]).astype(bf16), (row_id < col_id).astype(bf16), preferred_element_type=f32
    )
    facts = [
        route_ref[k : k + 1, :].astype(f32) * capacity + jnp.sum(named[k] * before, axis=0, keepdims=True)
        for k in range(2)
    ] + [share_ref[0:1, :], share_ref[1:2, :]]
    for k in range(4):
        info[k : k + 1, :] = facts[k]
    info[4:8, :] = jnp.zeros((4, rows), f32)
    spread = jnp.zeros((rows, rows), f32)
    for k in range(4):
        spread = jnp.where(row_id == k, facts[k], spread)
    cols_ref[...] = spread.T
    info_copy(my_slot).start()

    columns(1)
    sides(0)
    in_start(0, 2 * ny)
    if nz > 2:
        columns(2)
    in_start(1)
    in_start(2)
    sides(1)
    for dz in range(3, nz):
        columns(dz)

    scale = math.log2(math.e) / math.sqrt(head)
    later = (row_id > col_id).astype(bf16)
    later_all = jnp.concatenate([later, jnp.ones((rows, rows), bf16)], axis=1)
    summing = jnp.concatenate([later_all, later_all], axis=0)
    log2e = math.log2(math.e)
    chunk = 2 * rows

    for copy in own[2:]:
        copy.wait()

    def weigh(b):
        for h in range(heads_here):
            lanes = slice(h * head, (h + 1) * head)
            key = kbuf[b * rows : (b + 1) * rows, lanes]
            for start in range(b * rows, n * rows, chunk):
                stop = min(start + chunk, n * rows)
                score = lax.dot_general(
                    qbuf[start:stop, lanes], key, (((1,), (1,)), ((), ())), preferred_element_type=f32
                ) * scale
                tail = jnp.log(1.0 + jnp.exp2(-jnp.abs(score))) * log2e
                soft = jnp.maximum(score, 0.0) + tail
                log_sigmoid = jnp.minimum(score, 0.0) - tail
                if start == b * rows:
                    inside = lax.broadcasted_iota(jnp.int32, soft.shape, 1) < lax.broadcasted_iota(
                        jnp.int32, soft.shape, 0
                    )
                    soft = jnp.where(inside, soft, 0.0)
                high = soft.astype(bf16)
                low = (soft - high.astype(f32)).astype(bf16)
                sums = jnp.dot(jnp.concatenate([high, low], axis=1), summing, preferred_element_type=f32)
                part = log_sigmoid - sums[:, :rows]
                fresh = rows if start == b * rows else 0
                if fresh < stop - start:
                    carry = carry_ref[h, start + fresh : stop, :]
                    if fresh:
                        carry = jnp.concatenate([jnp.zeros((fresh, rows), f32), carry], axis=0)
                    part = part - carry
                    total = sums[:, rows:] + carry
                else:
                    total = sums[:, rows:]
                weight = jnp.exp2(part)
                if start == b * rows:
                    weight = jnp.where(inside, weight, 0.0)
                weight_ref[h, start:stop, b * rows : (b + 1) * rows] = weight.astype(bf16)
                if b > 0:
                    carry_ref[h, start:stop, :] = total

    for b in range(n - 1, -1, -1):
        in_wait(0, b)
        in_wait(1, b)
        weigh(b)
        if b == n // 2 and nz > 2:
            sides(2)
    for dz in range(3, nz):
        sides(dz)
    def o_copy(d):
        return pltpu.make_async_remote_copy(
            src_ref=osend.at[d], dst_ref=obuf.at[me],
            send_sem=o_send.at[d], recv_sem=o_recv.at[me],
            device_id=peer(d, dp), device_id_type=MESH,
        )

    for d in range(n):
        in_wait(2, d)
        for h in range(heads_here):
            lanes = slice(h * head, (h + 1) * head)
            osend[d, :, lanes] = jnp.dot(
                weight_ref[h, d * rows : (d + 1) * rows, : (d + 1) * rows],
                vbuf[: (d + 1) * rows, lanes],
                preferred_element_type=f32,
            ).astype(bf16)

    obuf[me] = osend[me]

    @pl.loop(1, n)
    def _(off):
        o_copy(flipped(me, n - off, n)).start()

    for off in range(1, n):
        for o in range(1, nx):
            beyond(off, o)
    for off in range(1, n):
        i = lax.rem(me + off, n)
        for x_off in range(nx):
            w_wait(None, lax.rem(x + x_off, nx) * cores + lax.rem(core + 1, cores), i)
    for load in loads:
        load.wait()

    acc[...] = res_ref[...].astype(f32)

    @pl.loop(0, n)
    def _(step):
        origin = flipped(me, step, n)

        @pl.when(step > 0)
        def _():
            pltpu.make_async_remote_copy(
                src_ref=osend.at[0], dst_ref=obuf.at[origin],
                send_sem=o_send.at[0], recv_sem=o_recv.at[origin],
                device_id=peer(origin, dp), device_id_type=MESH,
            ).wait_recv()

        block = obuf[origin]
        for q in range(m):
            part = slice(q * wcols, (q + 1) * wcols)
            acc[:, part] += jnp.dot(block, wbuf[q, origin], preferred_element_type=f32)

    square = jnp.zeros((rows, 1), f32)
    for q in range(m):
        part = slice(q * wcols, (q + 1) * wcols)
        stream = acc[:, part].astype(bf16)
        stream_ref[:, part] = stream
        stream = stream.astype(f32)
        acc[:, part] = stream
        square = square + jnp.sum(stream * stream, axis=1, keepdims=True)
    factor = lax.rsqrt(square / width + EPS)
    for q in range(m):
        part = slice(q * wcols, (q + 1) * wcols)
        normed_ref[:, part] = (acc[:, part] * factor * gain_ref[:, part]).astype(bf16)

    def chosen(facts, expert):
        slot = lax.broadcasted_iota(jnp.int32, (capacity, rows), 0) + expert * capacity
        slot = slot.astype(f32)
        return jnp.logical_or(facts[0:1, :] == slot, facts[1:2, :] == slot).astype(bf16)

    def there(off):
        return pltpu.make_async_remote_copy(
            src_ref=outgoing.at[off], dst_ref=inbox.at[off],
            send_sem=there_send.at[off], recv_sem=there_recv.at[off],
            device_id=peer(flipped(me, off, n), dp), device_id_type=MESH,
        )

    def arrival(off):
        return pltpu.make_async_remote_copy(
            src_ref=outgoing.at[0], dst_ref=inbox.at[off],
            send_sem=there_send.at[0], recv_sem=there_recv.at[off],
            device_id=peer(mate, dp), device_id_type=MESH,
        )

    def relay(slot, off, i):
        part = slice(i * lump, (i + 1) * lump)
        index = flipped(off, slot_of[slot], n)
        return pltpu.make_async_remote_copy(
            src_ref=relay_out.at[slot, off, :, part], dst_ref=inbox.at[index, :, part],
            send_sem=relay_send.at[slot, i, off], recv_sem=there_recv.at[index],
            device_id=peer(flipped(me, off, n), dp), device_id_type=MESH,
        )

    def home(off):
        return pltpu.make_async_remote_copy(
            src_ref=outbox.at[off], dst_ref=back.at[off],
            send_sem=back_send.at[off], recv_sem=back_recv.at[off],
            device_id=peer(flipped(me, off, n), dp), device_id_type=MESH,
        )

    hidden_width = gate_ref.shape[1]
    pieces = part_send.shape[1]
    piece = width // pieces
    hidden_piece = min(512, hidden_width)

    def via(off, slot, to, i):
        part = slice(i * piece, (i + 1) * piece)
        return pltpu.make_async_remote_copy(
            src_ref=outbox.at[off, :, part], dst_ref=relay_in.at[slot, to, :, part],
            send_sem=back_send.at[off], recv_sem=via_recv.at[slot, to, i],
            device_id=peer(flipped(me, to, n), dp), device_id_type=MESH,
        )

    def part_copy(slot, i):
        part = slice(i * piece, (i + 1) * piece)
        return pltpu.make_async_remote_copy(
            src_ref=partial_ref.at[slot, :, part], dst_ref=part_ref.at[:, part],
            send_sem=part_send.at[slot, i], recv_sem=part_recv.at[i],
            device_id=peer(flipped(me, slot_of[slot], n), dp), device_id_type=MESH,
        )

    def pack(off):
        outgoing[off] = jnp.dot(
            chosen(info, flipped(me, off, n)), normed_ref[...], preferred_element_type=f32
        ).astype(bf16)
        there(off).start()

    def pass_on(slot, chunks):
        if chunks[0] == 0:
            info_copy(slot).wait_recv()
        for i in chunks:
            part = slice(i * lump, (i + 1) * lump)
            raw_copy(slot, i).wait_recv()

            @pl.loop(1, span)
            def _(step):
                off = span - step
                relay_out[slot, off, :, part] = jnp.dot(
                    chosen(mate_info.at[slot], flipped(me, off, n)), raw_ref[slot, :, part],
                    preferred_element_type=f32,
                ).astype(bf16)
                relay(slot, off, i).start()

            inbox[slot_of[slot], :, part] = jnp.dot(
                chosen(mate_info.at[slot], me), raw_ref[slot, :, part], preferred_element_type=f32
            ).astype(bf16)

    @pl.when(inner)
    def _():
        for i in range(lumps):
            raw_copy(1, i).start()

    pl.loop(1, span)(pack)

    @pl.when(edge)
    def _():
        for i in range(lumps):
            raw_copy(0, i).start()

    inbox[0] = jnp.dot(chosen(info, me), normed_ref[...], preferred_element_type=f32).astype(bf16)

    @pl.when(inner)
    def _():
        pass_on(1, range(1))

    @pl.loop(0, pairs)
    def _(step):
        part_of, rest = step // (ny // 2), lax.rem(step, ny // 2)
        swapped = jnp.where(part_of == 2, 3, jnp.where(part_of == 3, 2, part_of))
        part_of = jnp.where(inner, swapped, part_of)
        even = part_of * ny + rest * 2
        odd = even + 1
        far = part_of >= half
        local = jnp.logical_or(even == 0, jnp.logical_and(inner, jnp.logical_and(far, rest == 0)))

        @pl.when(jnp.logical_and(inner, step == pairs // 4))
        def _():
            pass_on(1, range(1, lumps - 1))

        @pl.when(jnp.logical_and(inner, step == pairs // 2))
        def _():
            pass_on(1, range(lumps - 1, lumps))
            pass_on(0, range(lumps))
            for off in range(ny, span):
                home(off).start()

        @pl.when(jnp.logical_not(local))
        def _():
            arrival(even).wait_recv()

        arrival(odd).wait_recv()
        arrived = inbox[pl.ds(even, 2)].reshape(2 * capacity, width)
        hidden = []
        for first in range(0, hidden_width, hidden_piece):
            part = slice(first, first + hidden_piece)
            gate = jnp.dot(arrived, gate_ref[:, part], preferred_element_type=f32)
            upper = jnp.dot(arrived, up_ref[:, part], preferred_element_type=f32)
            hidden.append((jax.nn.silu(gate) * upper).astype(bf16))
        hidden = jnp.concatenate(hidden, axis=1)
        slot = jnp.where(inner, part_of - half, nz - 1 - part_of)
        to = jnp.where(inner, 0, ny) + rest * 2
        for i in range(pieces):
            part = slice(i * piece, (i + 1) * piece)
            result = jnp.dot(hidden, down_ref[:, part], preferred_element_type=f32)
            outbox[pl.ds(even, 2), :, part] = result.astype(bf16).reshape(2, capacity, piece)

            @pl.when(far)
            def _():
                @pl.when(jnp.logical_not(local))
                def _():
                    via(even, slot, to, i).start()

                via(odd, slot, to + 1, i).start()

        @pl.when(even == 0)
        def _():
            back[0] = outbox[0]

        held = jnp.logical_and(inner, part_of == 1)

        @pl.when(jnp.logical_not(jnp.logical_or(far, held)))
        def _():
            @pl.when(even > 0)
            def _():
                home(even).start()

            home(odd).start()

        @pl.when(far)
        def _():
            @pl.when(local)
            def _():
                relay_in[slot, 0] = outbox[even]


    def picks(facts, even, odd):
        slot = lax.broadcasted_iota(jnp.int32, (rows, 2 * capacity), 1)
        slot = jnp.where(slot < capacity, slot + even * capacity, slot - capacity + odd * capacity)
        slot = slot.astype(f32)
        return [(facts[:, k : k + 1] == slot).astype(bf16) for k in range(2)]

    def shared(facts, pick, block):
        first, second = [jnp.dot(pick[k], block, preferred_element_type=f32) for k in range(2)]
        return facts[:, 2:3] * first + facts[:, 3:4] * second

    @pl.when(inner)
    def _():
        for slot in range(2):
            spread = jnp.zeros((rows, rows), f32)
            for k in range(4):
                spread = jnp.where(row_id == k, mate_info[slot, k : k + 1, :], spread)
            mate_cols[slot] = spread.T

    @pl.loop(0, span // 2)
    def _(pair):
        @pl.when(pair > 0)
        def _():
            home(pair * 2).wait_recv()

        home(pair * 2 + 1).wait_recv()
        pick = picks(cols_ref, flipped(me, pair * 2, n), flipped(me, pair * 2 + 1, n))
        for start in range(0, width, piece):
            part = slice(start, start + piece)
            block = back[pl.ds(pair * 2, 2), :, part].reshape(2 * capacity, piece)
            acc[:, part] += shared(cols_ref, pick, block)

    @pl.when(inner)
    def _():
        for slot in (1, 0):
            facts = mate_cols.at[slot]
            pick = [picks(facts, flipped(me, p * 2, n), flipped(me, p * 2 + 1, n)) for p in range(span // 2)]
            for i in range(pieces):
                part = slice(i * piece, (i + 1) * piece)

                @pl.loop(1, span)
                def _(to):
                    via(0, slot, to, i).wait_recv()

                total = jnp.zeros((rows, piece), f32)
                for p in range(span // 2):
                    block = relay_in[slot, p * 2 : p * 2 + 2, :, part].reshape(2 * capacity, piece)
                    total = total + shared(facts, pick[p], block)
                partial_ref[slot, :, part] = total.astype(bf16)
                part_copy(slot, i).start()

    for i in range(pieces):
        part = slice(i * piece, (i + 1) * piece)
        part_copy(0, i).wait_recv()
        acc[:, part] += part_ref[:, part].astype(f32)

    out_ref[...] = acc[...].astype(bf16)

    for t in range(3):
        for off in range(1, n):
            in_copy(t, off).wait_send()
    @pl.loop(1, n)
    def _(off):
        o_copy(flipped(me, off, n)).wait_send()

    for cond, copy in sent:
        if cond is None:
            copy.wait_send()
        else:
            pl.when(cond)(copy.wait_send)

    info_copy(my_slot).wait_send()
    for i in range(lumps):
        raw_copy(my_slot, i).wait_send()

    @pl.loop(1, span)
    def _(off):
        there(off).wait_send()

    @pl.loop(1, n)
    def _(off):
        @pl.when(jnp.logical_or(edge, jnp.logical_and(off != slot_of[0], off != slot_of[1])))
        def _():
            pltpu.make_async_remote_copy(
                src_ref=outbox.at[off], dst_ref=inbox.at[off],
                send_sem=back_send.at[off], recv_sem=there_recv.at[off],
                device_id=peer(mate, dp), device_id_type=MESH,
            ).wait_send()

    @pl.when(inner)
    def _():
        for slot in range(2):
            for i in range(lumps):
                @pl.loop(1, span)
                def _(off):
                    relay(slot, off, i).wait_send()

            for i in range(pieces):
                part_copy(slot, i).wait_send()


def layer(queries, keys, values, proj_weight, residual, norm_gain, route, share, w_gate, w_up, w_down):
    n, m = lax.axis_size("sp"), lax.axis_size("dp")
    rows, width = queries.shape
    cols = width // n
    ny = 1 << ((n.bit_length() - 1) // 2)
    nz, nx = n // ny, m // 2
    copies = 1 + ny + 2 * nz * (ny + nx + 1) + (2 * nz) * ny * nx + n * nx
    capacity = 4 * rows // n
    hidden = w_gate.shape[2]
    heads_here = cols // (width // HEADS)
    bf16, f32 = jnp.bfloat16, jnp.float32
    lumps = 4
    return pl.pallas_call(
        functools.partial(layer_kernel, n, m, ny),
        out_shape=jax.ShapeDtypeStruct((rows, width), bf16),
        in_specs=[pl.BlockSpec(memory_space=pl.ANY)] * 11,
        out_specs=pl.BlockSpec(memory_space=pltpu.VMEM),
        scratch_shapes=[
            pltpu.VMEM((n * rows, cols), bf16),
            pltpu.VMEM((n * rows, cols), bf16),
            pltpu.VMEM((n * rows, cols), bf16),
            pltpu.VMEM((m, n, cols, width // m), bf16),
            pltpu.VMEM((n, rows, cols), bf16),
            pltpu.VMEM((n, rows, cols), bf16),
            pltpu.VMEM((heads_here, n * rows, n * rows), bf16),
            pltpu.VMEM((heads_here, n * rows, rows), f32),
            pltpu.VMEM((rows, width), f32),
            pltpu.VMEM((rows, width), bf16),
            pltpu.VMEM((rows, width), bf16),
            pltpu.VMEM((rows, width), bf16),
            pltpu.VMEM((1, width), f32),
            pltpu.VMEM((2, rows), jnp.int32),
            pltpu.VMEM((2, rows), f32),
            pltpu.VMEM((8, rows), f32),
            pltpu.VMEM((rows, rows), f32),
            pltpu.VMEM((width, hidden), bf16),
            pltpu.VMEM((width, hidden), bf16),
            pltpu.VMEM((hidden, width), bf16),
            pltpu.VMEM((n // 2, capacity, width), bf16),
            pltpu.VMEM((n, capacity, width), bf16),
            pltpu.VMEM((n, capacity, width), bf16),
            pltpu.VMEM((n // 2, capacity, width), bf16),
            pltpu.VMEM((2, rows, width), bf16),
            pltpu.VMEM((2, n // 2, capacity, width), bf16),
            pltpu.VMEM((2, n // 2, capacity, width), bf16),
            pltpu.VMEM((2, rows, width), bf16),
            pltpu.VMEM((rows, width), bf16),
            pltpu.VMEM((2, 8, rows), f32),
            pltpu.VMEM((2, rows, rows), f32),
            pltpu.SemaphoreType.DMA((5,)),
            pltpu.SemaphoreType.DMA((5 + m,)),
            pltpu.SemaphoreType.DMA((3, n)),
            pltpu.SemaphoreType.DMA((3, n)),
            pltpu.SemaphoreType.DMA((n,)),
            pltpu.SemaphoreType.DMA((n,)),
            pltpu.SemaphoreType.DMA((copies,)),
            pltpu.SemaphoreType.DMA((m, n)),
            pltpu.SemaphoreType.DMA((n,)),
            pltpu.SemaphoreType.DMA((n,)),
            pltpu.SemaphoreType.DMA((n,)),
            pltpu.SemaphoreType.DMA((n,)),
            pltpu.SemaphoreType.DMA((1,)),
            pltpu.SemaphoreType.DMA((2,)),
            pltpu.SemaphoreType.DMA((lumps,)),
            pltpu.SemaphoreType.DMA((2, lumps)),
            pltpu.SemaphoreType.DMA((2, lumps, n // 2)),
            pltpu.SemaphoreType.DMA((2, n // 2, 2 * lumps)),
            pltpu.SemaphoreType.DMA((2, 2 * lumps)),
            pltpu.SemaphoreType.DMA((2 * lumps,)),
        ],
        compiler_params=pltpu.CompilerParams(
            collective_id=0, has_side_effects=True, vmem_limit_bytes=50 * 1024 * 1024
        ),
    )(
        queries, keys, values, proj_weight, residual, norm_gain.reshape(1, width),
        route.T, share.T, w_gate, w_up, w_down,
    )


def body(
    queries,
    keys,
    values,
    proj_weight,
    residual,
    norm_gain,
    route,
    route_weight,
    w_gate,
    w_up,
    w_down,
):
    return layer(
        queries[0], keys[0], values[0], proj_weight, residual[0], norm_gain,
        route[0], route_weight[0], w_gate, w_up, w_down,
    )[None]


def solution(mesh):
    return jax.shard_map(
        body,
        mesh=mesh,
        in_specs=(
            P("dp", "sp", None),
            P("dp", "sp", None),
            P("dp", "sp", None),
            P("sp", None),
            P("dp", "sp", None),
            P(),
            P("dp", "sp", None),
            P("dp", "sp", None),
            P("sp", None, None),
            P("sp", None, None),
            P("sp", None, None),
        ),
        out_specs=P("dp", "sp", None),
        check_vma=False,
    )
```
